512 devices in a mesh: ep: 32 (over z, x), tp: 16 (over y, core).
Axes of the slice: x: 4, y: 8, z: 8, core: 2. Of those that a mesh axis runs over, the one named last changes fastest.
Arguments:
- tokens: bfloat16 [256, 2048], P('ep', 'tp'), may hold values from -10 to 10, as said below
- norm_gain: float32 [2048], P('tp'), may hold values from 0.5 to 1.5
- norm_bias: float32 [2048], P('tp'), may hold values from -0.3 to 0.3
- group_pick: int32 [256, 1], P('ep'), may hold values from 0 to 7; in each aligned block of 8 rows (0 to 7, 8 to 15, ...) at most 2 rows name the same one
- member_pick: int32 [256, 4], P('ep'), may hold values from 0 to 7, all different within a row
- picked_probs: float32 [256, 4], P('ep'), may hold values from 0.05 to 1
- gate_weight: bfloat16 [64, 2048, 1024], P('ep', 'tp'), may hold values from -0.125 to 0.125
- up_weight: bfloat16 [64, 2048, 1024], P('ep', 'tp'), may hold values from -0.125 to 0.125
- down_weight: bfloat16 [64, 1024, 2048], P('ep', None, 'tp'), may hold values from -0.375 to 0.375
Outputs:
- mixed: bfloat16 [256, 2048], P('ep', 'tp')
The draws below stay inside these ranges and needn't reach their ends.
Inputs may be any that keep to these rules, and one draw needn't show every extreme that they name: `group_pick`: each entry is a group number from 0 to 7; within each aligned block of 8 tokens no group is named by more than 2 tokens, a bound that some block reaches. `member_pick`: each token's 4 entries are different member numbers from 0 to 7. `tokens`: each token is its own offset between -2 and 2 plus its own scale between 0.25 and 2 times entries of at most 4 in size.
All inputs are finite; a program needn't handle non-finite values.
Results may differ from the reference program's by a relative error of at most 0.01.
Values may be sent and summed in bfloat16 or wider, within the bound.
No kernel may reach another device: no remote copies, remote signals or barrier semaphores. Data moves between devices by JAX's collectives and lax.ppermute only.
A program may use at most 64 MiB of HBM per device.

```python
import math
import jax
import jax.numpy as jnp
import numpy as np
from jax import lax

D = 2048
FF = 1024
EPG = 8
TOP_K = 4
TOK_DEV = 8
TOKENS = 256
EXPERTS = 64
GROUPS = 8
GCAP = 2


def draw_tokens(key, part):
    offset_key, scale_key, noise_key = jax.random.split(key, 3)
    offsets = jax.random.uniform(offset_key, (TOKENS, 1), jnp.float32, -2.0, 2.0)
    logs = jax.random.uniform(scale_key, (TOKENS, 1), jnp.float32, math.log(0.5), math.log(2.0))
    noise = jnp.clip(jax.random.normal(noise_key, (TOKENS, D), jnp.float32), -4.0, 4.0)
    return (offsets + jnp.exp(logs) * noise).astype(jnp.bfloat16)


def level_of(key, extent, cuts, smallest, largest):
    def one(dim, parts):
        heights = jax.random.uniform(jax.random.fold_in(jax.random.fold_in(key, 6), dim), (parts,), jnp.float32, smallest / len(cuts), largest / len(cuts))
        return jnp.repeat(jnp.exp(heights), extent[dim] // parts).reshape((-1,) + (1,) * (len(extent) - dim - 1))

    factor_of = one(*cuts[0])
    for cut in cuts[1:]:
        factor_of = factor_of * one(*cut)
    return factor_of


def picks_of(stream_key, rows, count, top, lift):
    sequence = jax.random.permutation(jax.random.fold_in(stream_key, 1), count)
    favour = sequence
    for power in range(3):
        favour = favour * favour // count
    favour = favour * lift // count
    tickets = jax.random.randint(jax.random.fold_in(stream_key, 2), (rows, count), 0, 4096) + favour
    fixed_rows = jax.random.permutation(jax.random.fold_in(stream_key, 3), rows)[jnp.arange(count) % rows]
    tickets = jnp.where(jnp.arange(rows)[:, None] == fixed_rows[None, :], 1 << 14, tickets)
    score = tickets * count + jnp.arange(count)
    return lax.top_k(score.astype(jnp.int32), top)[1].astype(jnp.int32)


def routed_block(stream_key, own, number, rows, number_of, top, most, lean):
    ranking = jax.random.permutation(stream_key, number_of)
    heavy_load, usual = portions_of(number_of, rows * top, most, lean, True), portions_of(number_of, rows * top, most, lean, False)
    places = jnp.arange(number_of)

    def named(tallies, turn):
        used = int((tallies > 0).sum())
        fixed = max(1, used // 4)
        moved = fixed + (places - fixed + turn * (used - fixed)) % max(1, number_of - fixed)
        return jnp.zeros((number_of,), jnp.int32).at[ranking[jnp.where(places < fixed, places, moved)]].set(jnp.asarray(tallies, jnp.int32))

    tallies = jnp.where(number % 4 == 0, named(heavy_load, number // 4), named(usual, number - number // 4 - 1))
    mixed = jax.random.permutation(jax.random.fold_in(own, 3), number_of)
    source_of, sink = mixed[0:number_of // 2 * 2:2], mixed[1:number_of // 2 * 2:2]
    room = jnp.minimum(tallies[source_of] - 1, most - tallies[sink]) // 2
    room = jnp.where((source_of == ranking[0]) | (sink == ranking[0]) | (tallies[sink] == 0), 0, jnp.maximum(room, 0))
    moved = jax.random.randint(jax.random.fold_in(own, 4), (number_of // 2,), 0, 1 << 20) % (room + 1)
    tallies = tallies.at[source_of].add(-moved).at[sink].add(moved)
    items = jnp.searchsorted(jnp.cumsum(tallies), jnp.arange(rows * top), side="right").astype(jnp.int32)
    grid = items.reshape(top, rows).T
    grid = grid[jax.random.permutation(jax.random.fold_in(own, 1), rows)]
    turn = jax.random.randint(jax.random.fold_in(own, 2), (rows, 1), 0, top)
    return jnp.take_along_axis(grid, (jnp.arange(top)[None, :] + turn) % top, axis=1)


def portions_of(amount, total, bound, lean, full):
    portions = [(1 << 20) // math.isqrt(standing ** lean) + 1 for standing in range(1, amount + 1)]
    largest = bound if full else min(bound, max(-(-total // amount), total * portions[0] // sum(portions)))
    least = 1 if total - largest >= amount - 1 else 0
    given, surplus = [largest] + [least] * (amount - 1), total - largest - least * (amount - 1)
    while surplus > 0:
        free = [i for i in range(1, amount) if given[i] < largest] or [i for i in range(1, amount) if given[i] < bound]
        whole, left = sum([portions[i] for i in free]), surplus
        for i in free:
            extra = min(bound - given[i], max(1, left * portions[i] // whole), surplus)
            given[i] = given[i] + extra
            surplus = surplus - extra
    return np.array(given)


def scatter_about(stream_key, dims, scale, limit, cuts=(), held_as=jnp.bfloat16):
    factor_of = level_of(stream_key, dims, cuts, -0.22, 0.18) if cuts else 1.0
    drawn = jax.random.normal(stream_key, dims, jnp.float32) * scale * factor_of
    return jnp.minimum(jnp.maximum(drawn, -limit), limit).astype(held_as)


def setup_inputs(seed: int = 0) -> dict:
    arg_keys = jax.random.split(jax.random.key(seed), 10)
    tokens = draw_tokens(jax.random.fold_in(arg_keys[9], 71), 0)
    norm_gain = jnp.clip(1.0 + 0.1 * jax.random.normal(arg_keys[1], (D,), jnp.float32), 0.5, 1.5)
    norm_bias = scatter_about(arg_keys[2], (D,), 0.1, 0.3, ((0, 16),), jnp.float32)
    group_pick_keys = jax.random.split(jax.random.fold_in(arg_keys[3], 1), TOKENS // TOK_DEV)
    group_pick_turns = jax.random.permutation(jax.random.fold_in(arg_keys[3], 3), TOKENS // TOK_DEV)
    group_pick = jax.vmap(lambda own, number: routed_block(jax.random.fold_in(arg_keys[3], 2), own, number, TOK_DEV, GROUPS, 1, GCAP, 2))(group_pick_keys, group_pick_turns).reshape((TOKENS, 1))
    member_pick = picks_of(arg_keys[4], TOKENS, EPG, TOP_K, 4096)
    picked_probs = jnp.clip(jnp.exp(math.log(1.0) - 2.9957323 * jax.random.uniform(arg_keys[5], (TOKENS, TOP_K), jnp.float32) ** level_of(arg_keys[5], (TOKENS, TOP_K), ((0, 32),), -0.2, 0.2)), 0.05, 1.0)
    gate_weight = scatter_about(arg_keys[6], (EXPERTS, D, FF), D ** -0.5, 0.125, ((0, 32), (1, 16)))
    up_weight = scatter_about(arg_keys[7], (EXPERTS, D, FF), D ** -0.5, 0.125, ((0, 32), (1, 16)))
    down_weight = scatter_about(arg_keys[8], (EXPERTS, FF, D), (FF // 4) ** -0.5, 0.375, ((0, 32), (2, 16)))
    return {"tokens": tokens, "norm_gain": norm_gain, "norm_bias": norm_bias, "group_pick": group_pick, "member_pick": member_pick, "picked_probs": picked_probs, "gate_weight": gate_weight, "up_weight": up_weight, "down_weight": down_weight}


norm_epsilon = 1e-5


def reference(tokens, norm_gain, norm_bias, group_pick, member_pick, picked_probs, gate_weight, up_weight, down_weight):
    values = tokens.astype(jnp.float32)
    center = jnp.mean(values, axis=1, keepdims=True)
    shifted = values - center
    spread = jnp.mean(shifted * shifted, axis=1, keepdims=True)
    scaled = shifted * lax.rsqrt(spread + norm_epsilon)
    normed = (scaled * norm_gain.astype(jnp.float32) + norm_bias.astype(jnp.float32)).astype(jnp.bfloat16)
    chosen = (group_pick * EPG + member_pick).astype(jnp.int32)
    shares = picked_probs / jnp.sum(picked_probs, axis=1, keepdims=True)

    def one_token(packed):
        row, picks, weights = packed
        row_wide = row.astype(jnp.float32)
        gate_rows = jnp.take(gate_weight, picks, axis=0).astype(jnp.float32)
        up_rows = jnp.take(up_weight, picks, axis=0).astype(jnp.float32)
        down_rows = jnp.take(down_weight, picks, axis=0).astype(jnp.float32)
        gate_sum = jnp.einsum("d,kdf->kf", row_wide, gate_rows)
        up_sum = jnp.einsum("d,kdf->kf", row_wide, up_rows)
        hidden = (jax.nn.silu(gate_sum) * up_sum).astype(jnp.bfloat16)
        expert_out = jnp.einsum("kf,kfd->kd", hidden.astype(jnp.float32), down_rows).astype(jnp.bfloat16)
        return jnp.sum(weights[:, None] * expert_out.astype(jnp.float32), axis=0)

    combined = lax.map(one_token, (normed, chosen, shares))
    return combined.astype(jnp.bfloat16)
```

```python
import functools

import jax
import jax.numpy as jnp
from jax import lax
from jax.experimental import pallas as pl
from jax.experimental.pallas import tpu as pltpu
from jax.sharding import Mesh
from jax.sharding import PartitionSpec as P

f32 = jnp.float32
bf16 = jnp.bfloat16

EPG = 8
SLOTS = 2
LANES = 128
NORM_EPSILON = 1e-05

VMEM = pl.BlockSpec(memory_space=pltpu.VMEM)
SMEM = pl.BlockSpec(memory_space=pltpu.SMEM)


def call(body, out_shape, in_specs, flops=0, moved=0):
    specs = jax.tree.map(lambda _: VMEM, out_shape)
    return pl.pallas_call(
        body,
        out_shape=out_shape,
        in_specs=in_specs,
        out_specs=specs,
        cost_estimate=pl.CostEstimate(flops=flops, bytes_accessed=moved, transcendentals=0),
    )


def shape(dims, dtype=bf16):
    return jax.ShapeDtypeStruct(dims, dtype)


def three(value):
    high = value.astype(bf16).astype(f32)
    middle = (value - high).astype(bf16).astype(f32)
    low = (value - high - middle).astype(bf16).astype(f32)
    return high, middle, low


def iota(dims, axis):
    return lax.broadcasted_iota(jnp.int32, dims, axis)


def by_row(rows, width):
    at = iota((8, width), 0)
    out = jnp.zeros((8, width), f32)
    for i, row in enumerate(rows):
        out = jnp.where(at == i, jnp.broadcast_to(row, (8, width)), out)
    return out


def dot(a, b):
    return jnp.dot(a, b, preferred_element_type=f32)


def slots_of(groups):
    count = groups.shape[1]
    at = iota((1, count), 1)
    slots = jnp.zeros((1, count), jnp.int32)
    for j in range(count - 1):
        same = jnp.broadcast_to(groups[:, j : j + 1], (1, count)) == groups
        slots = slots + jnp.where(same & (at > j), 1, 0)
    return slots


def share_body(tokens, gain, bias, out):
    out[0:8, :] = tokens[...]
    rows = three(gain[...]) + three(bias[...])
    out[8:16, :] = by_row(rows, LANES).astype(bf16)


def pack_body(core, both, groups, out, affine):
    first, second = both[0].astype(f32), both[1].astype(f32)
    lower = core[0] == 0
    own, other = jnp.where(lower, first, second), jnp.where(lower, second, first)
    affine[:, 0:LANES] = own[8:16].astype(bf16)
    affine[:, LANES:] = other[8:16].astype(bf16)
    values = jnp.concatenate([own[0:8], other[0:8]], axis=0).astype(bf16)
    place = out.shape[0]
    per = place // 8
    chosen = groups[...]
    slots = slots_of(chosen)
    pair = jnp.concatenate([chosen, chosen], axis=1)
    slot_pair = jnp.concatenate([slots, slots], axis=1)
    row = iota((place, 16), 0)
    half = jnp.where(iota((place, 16), 1) >= 8, 1, 0)
    hit = (
        (row // per == pair)
        & (row % SLOTS == slot_pair)
        & ((row // SLOTS) % 2 == half)
    )
    out[...] = dot(jnp.where(hit, 1.0, 0.0).astype(bf16), values).astype(bf16)


def spread_body(arrived, affine, own, received, out):
    places = arrived.shape[0]
    rows = places // 2
    at, source = iota((rows, places), 0), iota((rows, places), 1)
    values = arrived[...]
    halves = []
    for half in range(2):
        takes = source == (at // SLOTS) * (2 * SLOTS) + half * SLOTS + at % SLOTS
        halves.append(dot(jnp.where(takes, 1.0, 0.0).astype(bf16), values))
    features = 2 * LANES
    mean = (
        jnp.sum(halves[0], axis=1, keepdims=True) + jnp.sum(halves[1], axis=1, keepdims=True)
    ) / features
    centred = [h - mean for h in halves]
    square = jnp.sum(centred[0] * centred[0] + centred[1] * centred[1], axis=1, keepdims=True)

    lane = iota((rows, LANES), 1)
    stats = jnp.where(lane == 0, mean, jnp.where(lane == 1, square, 0.0))
    stats = jnp.concatenate([stats, jnp.zeros((LANES - rows, LANES), f32)], axis=0).T
    means, squares = three(stats[0:1]), three(stats[1:2])

    left = []
    for half in range(2):
        lanes = slice(half * LANES, (half + 1) * LANES)
        affine_rows = affine[:, lanes]
        wide = affine_rows.astype(f32)
        gain = wide[0:1] + wide[1:2] + wide[2:3]
        left.append(jnp.concatenate([(centred[half] * gain).astype(bf16), affine_rows], axis=0))

    for mat, stat in ((0, means), (1, squares)):
        total = dot(left[0], own[mat]) + dot(left[1], received[mat])
        tail = total[rows : rows + 8]
        gain_sum = tail[0:1] + tail[1:2] + tail[2:3]
        bias_sum = tail[3:4] + tail[4:5] + tail[5:6]
        parts = three(gain_sum)[0:2] + three(bias_sum)[0:2]
        for y in range(out.shape[0]):
            lanes = slice(y * LANES, (y + 1) * LANES)
            put = slice(mat * LANES, (mat + 1) * LANES)
            out[y, 0:rows, put] = total[0:rows, lanes].astype(bf16)
            out[y, rows : rows + 8, put] = by_row([p[:, lanes] for p in parts] + list(stat), LANES).astype(bf16)


def activate_body(features, parts, out):
    peers = parts.shape[0]
    rows = parts.shape[1] - 8
    tails = [parts[s, rows : rows + 8, :].astype(f32) for s in range(peers)]
    means = by_row([t[4:5, 0:LANES] + t[5:6, 0:LANES] + t[6:7, 0:LANES] for t in tails], LANES)
    squares = by_row([t[4:5, LANES:] + t[5:6, LANES:] + t[6:7, LANES:] for t in tails], LANES)
    center = jnp.sum(means, axis=0, keepdims=True) / peers
    shift = means - center
    spread = jnp.sum(squares + (features // peers) * shift * shift, axis=0, keepdims=True) / features
    scale = jnp.broadcast_to(lax.rsqrt(spread + NORM_EPSILON), (8, LANES))
    turned = jnp.concatenate([shift, scale, jnp.zeros((LANES - 16, LANES), f32)], axis=0).T

    sums = parts[0, 0:rows, :].astype(f32)
    for s in range(1, peers):
        sums = sums + parts[s, 0:rows, :].astype(f32)
    bias = tails[0][2:3] + tails[0][3:4]
    for s in range(peers):
        sums = sums + turned[0:rows, s : s + 1] * (tails[s][0:1] + tails[s][1:2])
        if s:
            bias = bias + tails[s][2:3] + tails[s][3:4]
    full = turned[0:rows, 8:9] * sums + bias
    gate, up = full[:, 0:LANES], full[:, LANES:]
    hidden = (gate / (1.0 + jnp.exp(-gate)) * up).astype(bf16)
    for s in range(peers):
        out[s] = hidden


def project_body(hidden, down, out):
    experts, tiles, rows, width = hidden.shape
    places = out.shape[0]
    row, source = iota((places, rows), 0), iota((places, rows), 1)
    total = jnp.zeros((places, LANES), f32)
    for e in range(experts):
        wide = jnp.concatenate([hidden[e, y] for y in range(tiles)], axis=1)
        result = dot(wide, down[e]).astype(bf16)
        puts = row == (source // SLOTS) * (2 * SLOTS) + e * SLOTS + source % SLOTS
        total = total + dot(jnp.where(puts, 1.0, 0.0).astype(bf16), result)
    out[...] = total.astype(bf16)


def combine_body(returned, groups, members, probs, out):
    places = returned.shape[0]
    count = groups.shape[1]
    chosen = groups[...]
    slots = slots_of(chosen)
    likely = probs[...]
    shares = likely / jnp.sum(likely, axis=0, keepdims=True)
    row = iota((places, count), 0)
    weights = jnp.zeros((places, count), f32)
    for k in range(members.shape[0]):
        member = members[k : k + 1, :]
        place = (chosen * (EPG // 2) + member // 2) * (2 * SLOTS) + (member % 2) * SLOTS + slots
        weights = weights + jnp.where(row == place, shares[k : k + 1, :], 0.0)
    values = returned[...]
    total = jnp.zeros((count, LANES), f32)
    for part in three(weights):
        total = total + lax.dot_general(
            part.astype(bf16), values, (((0,), (0,)), ((), ())), preferred_element_type=f32
        )
    out[...] = total.astype(bf16)


def on_device(
    tokens,
    norm_gain,
    norm_bias,
    group_pick,
    member_pick,
    picked_probs,
    gate_weight,
    up_weight,
    down_weight,
):
    ep = ("z", "x")
    peers = lax.axis_size(ep)
    tiles = lax.axis_size("y")
    count, width = tokens.shape
    inner = gate_weight.shape[2]
    rows = peers * SLOTS
    places = 2 * rows
    features = width * tiles * 2
    core = lax.axis_index("c")
    groups, members, probs = group_pick.T, member_pick.T, picked_probs.T

    pick = lambda w, i: lax.dynamic_index_in_dim(w, i, 0, keepdims=False)
    sent = jnp.stack([pick(gate_weight, 1 - core), pick(up_weight, 1 - core)])
    received = lax.ppermute(sent, "c", [(0, 1), (1, 0)])
    own = jnp.stack([pick(gate_weight, core), pick(up_weight, core)])

    mine = call(share_body, shape((16, LANES)), [VMEM] * 3)(
        tokens, norm_gain.reshape(1, width), norm_bias.reshape(1, width)
    )
    both = lax.all_gather(mine, "c", axis=0, tiled=False)
    outgoing, affine = call(
        pack_body, (shape((places, LANES)), shape((8, 2 * LANES))), [SMEM, VMEM, VMEM]
    )(core.reshape(1), both, groups)
    arrived = lax.all_to_all(
        outgoing.reshape(peers, 2 * SLOTS, LANES), ep, split_axis=0, concat_axis=0, tiled=True
    ).reshape(places, LANES)

    parts = call(
        spread_body,
        shape((tiles, rows + 8, 2 * LANES)),
        [VMEM] * 4,
        flops=2 * (rows + 8) * 2 * width * 2 * inner,
        moved=own.size * 4,
    )(arrived, affine, own, received)
    parts = lax.all_to_all(parts, "y", split_axis=0, concat_axis=0, tiled=True)
    hidden = call(functools.partial(activate_body, features), shape((tiles, rows, LANES)), [VMEM])(parts)
    hidden = lax.all_to_all(hidden, "y", split_axis=0, concat_axis=0, tiled=True)
    hidden = lax.all_gather(hidden, "c", axis=0, tiled=False)
    results = call(
        project_body,
        shape((places, LANES)),
        [VMEM] * 2,
        flops=2 * rows * 2 * inner * width,
        moved=down_weight.size * 2,
    )(hidden, down_weight)
    returned = lax.all_to_all(
        results.reshape(peers, 2 * SLOTS, LANES), ep, split_axis=0, concat_axis=0, tiled=True
    ).reshape(places, LANES)
    return call(combine_body, shape((count, LANES)), [VMEM] * 4)(returned, groups, members, probs)


def solution(mesh):
    finer = Mesh(mesh.devices.reshape(8, 4, 8, 2), ("z", "x", "y", "c"))
    ep, tp = ("z", "x"), ("y", "c")
    placed = (
        P(ep, tp),
        P(tp),
        P(tp),
        P(ep, None),
        P(ep, None),
        P(ep, None),
        P(ep, tp, None),
        P(ep, tp, None),
        P(ep, None, tp),
    )
    return jax.shard_map(
        on_device, mesh=finer, in_specs=placed, out_specs=P(ep, tp), check_vma=False
    )
```

```python
import functools

import jax
import jax.numpy as jnp
from jax import lax
from jax.experimental import pallas as pl
from jax.experimental.pallas import tpu as pltpu
from jax.sharding import Mesh
from jax.sharding import PartitionSpec as P

f32 = jnp.float32
bf16 = jnp.bfloat16

EPG = 8
SLOTS = 2
LANES = 128
NORM_EPSILON = 1e-05

VMEM = pl.BlockSpec(memory_space=pltpu.VMEM)
SMEM = pl.BlockSpec(memory_space=pltpu.SMEM)
ANY = pl.BlockSpec(memory_space=pl.ANY)


def call(body, out_shape, in_specs, flops=0, moved=0, scratch=()):
    specs = jax.tree.map(lambda _: VMEM, out_shape)
    kernel = pl.pallas_call(
        body,
        out_shape=out_shape,
        in_specs=in_specs,
        out_specs=specs,
        scratch_shapes=scratch,
        cost_estimate=pl.CostEstimate(flops=flops, bytes_accessed=moved, transcendentals=0),
    )

    def run(*args):
        near = [
            pltpu.with_memory_space_constraint(a, pltpu.VMEM) if spec is VMEM else a
            for a, spec in zip(args, in_specs)
        ]
        return kernel(*near)

    return run


def shape(dims, dtype=bf16):
    return pltpu.VMEM(dims, dtype)


def three(value):
    high = value.astype(bf16).astype(f32)
    middle = (value - high).astype(bf16).astype(f32)
    low = (value - high - middle).astype(bf16).astype(f32)
    return high, middle, low


def iota(dims, axis):
    return lax.broadcasted_iota(jnp.int32, dims, axis)


def by_row(rows, width):
    at = iota((8, width), 0)
    out = jnp.zeros((8, width), f32)
    for i, row in enumerate(rows):
        out = jnp.where(at == i, jnp.broadcast_to(row, (8, width)), out)
    return out


def dot(a, b):
    return jnp.dot(a, b, preferred_element_type=f32)


def slots_of(groups):
    count = groups.shape[1]
    at = iota((1, count), 1)
    slots = jnp.zeros((1, count), jnp.int32)
    for j in range(count - 1):
        same = jnp.broadcast_to(groups[:, j : j + 1], (1, count)) == groups
        slots = slots + jnp.where(same & (at > j), 1, 0)
    return slots


def share_body(core, tokens, gain, bias, groups, members, probs, gate, up, out, sent, hits, weights, *scratch):
    near_gain, near_bias, near_groups, near_members, near_probs, arrived = scratch
    peer = 1 - core[0]
    pairs = (
        (gain, near_gain),
        (bias, near_bias),
        (groups, near_groups),
        (members, near_members),
        (probs, near_probs),
        (tokens, out.at[0:8]),
        (gate.at[peer], sent.at[0]),
        (up.at[peer], sent.at[1]),
    )
    copies = [pltpu.make_async_copy(a, b, arrived.at[i]) for i, (a, b) in enumerate(pairs)]
    for copy in copies:
        copy.start()
    for copy in copies[0:5]:
        copy.wait()
    rows = three(near_gain[...]) + three(near_bias[...])
    out[8:16, :] = by_row(rows, LANES).astype(bf16)

    place = hits.shape[0]
    per = place // 8
    chosen = near_groups[...]
    slots = slots_of(chosen)
    pair = jnp.concatenate([chosen, chosen], axis=1)
    slot_pair = jnp.concatenate([slots, slots], axis=1)
    row = iota((place, 16), 0)
    half = jnp.where(iota((place, 16), 1) >= 8, 1, 0)
    hit = (
        (row // per == pair)
        & (row % SLOTS == slot_pair)
        & ((row // SLOTS) % 2 == half)
    )
    hits[...] = jnp.where(hit, 1.0, 0.0).astype(bf16)

    likely = near_probs[...]
    shares = likely / jnp.sum(likely, axis=0, keepdims=True)
    row = iota((place, 8), 0)
    total = jnp.zeros((place, 8), f32)
    for k in range(members.shape[0]):
        member = near_members[k : k + 1, :]
        at = (chosen * (EPG // 2) + member // 2) * (2 * SLOTS) + (member % 2) * SLOTS + slots
        total = total + jnp.where(row == at, shares[k : k + 1, :], 0.0)
    weights[...] = total
    for copy in copies[5:]:
        copy.wait()


def pack_body(core, both, hits, out, affine):
    first, second = both[0].astype(f32), both[1].astype(f32)
    lower = core[0] == 0
    own, other = jnp.where(lower, first, second), jnp.where(lower, second, first)
    affine[:, 0:LANES] = own[8:16].astype(bf16)
    affine[:, LANES:] = other[8:16].astype(bf16)
    values = jnp.concatenate([own[0:8], other[0:8]], axis=0).astype(bf16)
    out[...] = dot(hits[...], values).astype(bf16)


def spread_body(core, arrived, affine, gate, up, received, out):
    places = arrived.shape[0]
    rows = places // 2
    at, source = iota((rows, places), 0), iota((rows, places), 1)
    values = arrived[...]
    halves = []
    for half in range(2):
        takes = source == (at // SLOTS) * (2 * SLOTS) + half * SLOTS + at % SLOTS
        halves.append(dot(jnp.where(takes, 1.0, 0.0).astype(bf16), values))
    features = 2 * LANES
    mean = (
        jnp.sum(halves[0], axis=1, keepdims=True) + jnp.sum(halves[1], axis=1, keepdims=True)
    ) / features
    centred = [h - mean for h in halves]
    square = jnp.sum(centred[0] * centred[0] + centred[1] * centred[1], axis=1, keepdims=True)

    lane = iota((rows, LANES), 1)
    stats = jnp.where(lane == 0, mean, jnp.where(lane == 1, square, 0.0))
    stats = jnp.concatenate([stats, jnp.zeros((LANES - rows, LANES), f32)], axis=0).T
    means, squares = three(stats[0:1]), three(stats[1:2])

    left = []
    for half in range(2):
        lanes = slice(half * LANES, (half + 1) * LANES)
        affine_rows = affine[:, lanes]
        wide = affine_rows.astype(f32)
        gain = wide[0:1] + wide[1:2] + wide[2:3]
        left.append(jnp.concatenate([(centred[half] * gain).astype(bf16), affine_rows], axis=0))

    for mat, stat in ((0, means), (1, squares)):
        own = (gate, up)[mat][core[0]]
        total = dot(left[0], own) + dot(left[1], received[mat])
        tail = total[rows : rows + 8]
        gain_sum = tail[0:1] + tail[1:2] + tail[2:3]
        bias_sum = tail[3:4] + tail[4:5] + tail[5:6]
        parts = three(gain_sum)[0:2] + three(bias_sum)[0:2]
        for y in range(out.shape[0]):
            lanes = slice(y * LANES, (y + 1) * LANES)
            put = slice(mat * LANES, (mat + 1) * LANES)
            out[y, 0:rows, put] = total[0:rows, lanes].astype(bf16)
            out[y, rows : rows + 8, put] = by_row([p[:, lanes] for p in parts] + list(stat), LANES).astype(bf16)


def activate_body(features, parts, out):
    peers = parts.shape[0]
    rows = parts.shape[1] - 8
    tails = [parts[s, rows : rows + 8, :].astype(f32) for s in range(peers)]
    means = by_row([t[4:5, 0:LANES] + t[5:6, 0:LANES] + t[6:7, 0:LANES] for t in tails], LANES)
    squares = by_row([t[4:5, LANES:] + t[5:6, LANES:] + t[6:7, LANES:] for t in tails], LANES)
    center = jnp.sum(means, axis=0, keepdims=True) / peers
    shift = means - center
    spread = jnp.sum(squares + (features // peers) * shift * shift, axis=0, keepdims=True) / features
    scale = jnp.broadcast_to(lax.rsqrt(spread + NORM_EPSILON), (8, LANES))
    turned = jnp.concatenate([shift, scale, jnp.zeros((LANES - 16, LANES), f32)], axis=0).T

    sums = parts[0, 0:rows, :].astype(f32)
    for s in range(1, peers):
        sums = sums + parts[s, 0:rows, :].astype(f32)
    bias = tails[0][2:3] + tails[0][3:4]
    for s in range(peers):
        sums = sums + turned[0:rows, s : s + 1] * (tails[s][0:1] + tails[s][1:2])
        if s:
            bias = bias + tails[s][2:3] + tails[s][3:4]
    full = turned[0:rows, 8:9] * sums + bias
    gate, up = full[:, 0:LANES], full[:, LANES:]
    hidden = (gate / (1.0 + jnp.exp(-gate)) * up).astype(bf16)
    for s in range(peers):
        out[s] = hidden


def project_body(hidden, down, out):
    experts, tiles, rows, width = hidden.shape
    places = out.shape[0]
    row, source = iota((places, rows), 0), iota((places, rows), 1)
    total = jnp.zeros((places, LANES), f32)
    for e in range(experts):
        wide = jnp.concatenate([hidden[e, y] for y in range(tiles)], axis=1)
        result = dot(wide, down[e]).astype(bf16)
        puts = row == (source // SLOTS) * (2 * SLOTS) + e * SLOTS + source % SLOTS
        total = total + dot(jnp.where(puts, 1.0, 0.0).astype(bf16), result)
    out[...] = total.astype(bf16)


def combine_body(returned, weights, out):
    values = returned[...]
    total = jnp.zeros(out.shape, f32)
    for part in three(weights[...]):
        total = total + lax.dot_general(
            part.astype(bf16), values, (((0,), (0,)), ((), ())), preferred_element_type=f32
        )
    out[...] = total.astype(bf16)


def on_device(
    tokens,
    norm_gain,
    norm_bias,
    group_pick,
    member_pick,
    picked_probs,
    gate_weight,
    up_weight,
    down_weight,
):
    ep = ("z", "x")
    peers = lax.axis_size(ep)
    tiles = lax.axis_size("y")
    count, width = tokens.shape
    inner = gate_weight.shape[2]
    rows = peers * SLOTS
    places = 2 * rows
    features = width * tiles * 2
    core = lax.axis_index("c")
    groups, members, probs = group_pick.T, member_pick.T, picked_probs.T

    at = core.reshape(1)
    mine, sent, hits, weights = call(
        share_body,
        (
            shape((16, LANES)),
            shape((2, width, inner)),
            shape((places, 2 * count)),
            shape((places, count), f32),
        ),
        [SMEM] + [ANY] * 8,
        scratch=[
            pltpu.VMEM((1, width), f32),
            pltpu.VMEM((1, width), f32),
            pltpu.VMEM(groups.shape, groups.dtype),
            pltpu.VMEM(members.shape, members.dtype),
            pltpu.VMEM(probs.shape, probs.dtype),
            pltpu.SemaphoreType.DMA((8,)),
        ],
    )(
        at,
        tokens,
        norm_gain.reshape(1, width),
        norm_bias.reshape(1, width),
        groups,
        members,
        probs,
        gate_weight,
        up_weight,
    )
    received = lax.ppermute(sent, "c", [(0, 1), (1, 0)])
    both = lax.all_gather(mine, "c", axis=0, tiled=False)
    outgoing, affine = call(
        pack_body, (shape((places, LANES)), shape((8, 2 * LANES))), [SMEM] + [VMEM] * 2
    )(at, both, hits)
    arrived = lax.all_to_all(
        outgoing.reshape(peers, 2 * SLOTS, LANES), ep, split_axis=0, concat_axis=0, tiled=True
    ).reshape(places, LANES)

    parts = call(
        spread_body,
        shape((tiles, rows + 8, 2 * LANES)),
        [SMEM] + [VMEM] * 5,
        flops=2 * (rows + 8) * 2 * width * 2 * inner,
        moved=received.size * 4,
    )(at, arrived, affine, gate_weight, up_weight, received)
    parts = lax.all_to_all(parts, "y", split_axis=0, concat_axis=0, tiled=True)
    hidden = call(functools.partial(activate_body, features), shape((tiles, rows, LANES)), [VMEM])(parts)
    hidden = lax.all_to_all(hidden, "y", split_axis=0, concat_axis=0, tiled=True)
    hidden = lax.all_gather(hidden, "c", axis=0, tiled=False)
    results = call(
        project_body,
        shape((places, LANES)),
        [VMEM] * 2,
        flops=2 * rows * 2 * inner * width,
        moved=down_weight.size * 2,
    )(hidden, down_weight)
    returned = lax.all_to_all(
        results.reshape(peers, 2 * SLOTS, LANES), ep, split_axis=0, concat_axis=0, tiled=True
    ).reshape(places, LANES)
    return call(combine_body, jax.ShapeDtypeStruct((count, LANES), bf16), [VMEM] * 2)(returned, weights)


def solution(mesh):
    finer = Mesh(mesh.devices.reshape(8, 4, 8, 2), ("z", "x", "y", "c"))
    ep, tp = ("z", "x"), ("y", "c")
    placed = (
        P(ep, tp),
        P(tp),
        P(tp),
        P(ep, None),
        P(ep, None),
        P(ep, None),
        P(ep, tp, None),
        P(ep, tp, None),
        P(ep, None, tp),
    )
    return jax.shard_map(
        on_device, mesh=finer, in_specs=placed, out_specs=P(ep, tp), check_vma=False
    )
```

```python
import functools

import jax
import jax.numpy as jnp
from jax import lax
from jax.experimental import pallas as pl
from jax.experimental.pallas import tpu as pltpu
from jax.sharding import Mesh
from jax.sharding import PartitionSpec as P


f32 = jnp.float32
bf16 = jnp.bfloat16

EPG = 8
SLOTS = 2
LANES = 128
NORM_EPSILON = 1e-05

VMEM = pl.BlockSpec(memory_space=pltpu.VMEM)
SMEM = pl.BlockSpec(memory_space=pltpu.SMEM)
ANY = pl.BlockSpec(memory_space=pl.ANY)


def call(body, out_shape, in_specs, flops=0, moved=0, scratch=()):
    specs = jax.tree.map(lambda _: VMEM, out_shape)
    kernel = pl.pallas_call(
        body,
        out_shape=out_shape,
        in_specs=in_specs,
        out_specs=specs,
        scratch_shapes=scratch,
        cost_estimate=pl.CostEstimate(flops=flops, bytes_accessed=moved, transcendentals=0),
    )

    def run(*args):
        near = [
            pltpu.with_memory_space_constraint(a, pltpu.VMEM) if spec is VMEM else a
            for a, spec in zip(args, in_specs)
        ]
        return kernel(*near)

    return run


def shape(dims, dtype=bf16):
    return pltpu.VMEM(dims, dtype)


def three(value):
    high = value.astype(bf16).astype(f32)
    middle = (value - high).astype(bf16).astype(f32)
    low = (value - high - middle).astype(bf16).astype(f32)
    return high, middle, low


def iota(dims, axis):
    return lax.broadcasted_iota(jnp.int32, dims, axis)


def by_row(rows, width):
    at = iota((8, width), 0)
    out = jnp.zeros((8, width), f32)
    for i, row in enumerate(rows):
        out = jnp.where(at == i, jnp.broadcast_to(row, (8, width)), out)
    return out


def dot(a, b):
    return jnp.dot(a, b, preferred_element_type=f32)


def slots_of(groups):
    count = groups.shape[1]
    at = iota((1, count), 1)
    slots = jnp.zeros((1, count), jnp.int32)
    for j in range(count - 1):
        same = jnp.broadcast_to(groups[:, j : j + 1], (1, count)) == groups
        slots = slots + jnp.where(same & (at > j), 1, 0)
    return slots


def slice_body(core, gate, up, sent, arrived):
    peer = 1 - core[0]
    copies = [
        pltpu.make_async_copy(gate.at[peer], sent.at[0], arrived.at[0]),
        pltpu.make_async_copy(up.at[peer], sent.at[1], arrived.at[1]),
    ]
    for copy in copies:
        copy.start()
    for copy in copies:
        copy.wait()


def share_body(tokens, gain, bias, groups, members, probs, out, hits, weights, *scratch):
    near_gain, near_bias, near_groups, near_members, near_probs, arrived = scratch
    pairs = (
        (gain, near_gain),
        (bias, near_bias),
        (groups, near_groups),
        (members, near_members),
        (probs, near_probs),
        (tokens, out.at[0:8]),
    )
    copies = [pltpu.make_async_copy(a, b, arrived.at[i]) for i, (a, b) in enumerate(pairs)]
    for copy in copies:
        copy.start()
    for copy in copies[0:5]:
        copy.wait()
    rows = three(near_gain[...]) + three(near_bias[...])
    out[8:16, :] = by_row(rows, LANES).astype(bf16)

    place = hits.shape[0]
    per = place // 8
    chosen = near_groups[...]
    slots = slots_of(chosen)
    pair = jnp.concatenate([chosen, chosen], axis=1)
    slot_pair = jnp.concatenate([slots, slots], axis=1)
    row = iota((place, 16), 0)
    half = jnp.where(iota((place, 16), 1) >= 8, 1, 0)
    hit = (
        (row // per == pair)
        & (row % SLOTS == slot_pair)
        & ((row // SLOTS) % 2 == half)
    )
    hits[...] = jnp.where(hit, 1.0, 0.0).astype(bf16)

    likely = near_probs[...]
    shares = likely / jnp.sum(likely, axis=0, keepdims=True)
    row = iota((place, 8), 0)
    total = jnp.zeros((place, 8), f32)
    for k in range(members.shape[0]):
        member = near_members[k : k + 1, :]
        at = (chosen * (EPG // 2) + member // 2) * (2 * SLOTS) + (member % 2) * SLOTS + slots
        total = total + jnp.where(row == at, shares[k : k + 1, :], 0.0)
    weights[...] = total
    for copy in copies[5:]:
        copy.wait()


def pack_body(core, both, hits, out, affine):
    first, second = both[0].astype(f32), both[1].astype(f32)
    lower = core[0] == 0
    own, other = jnp.where(lower, first, second), jnp.where(lower, second, first)
    affine[:, 0:LANES] = own[8:16].astype(bf16)
    affine[:, LANES:] = other[8:16].astype(bf16)
    values = jnp.concatenate([own[0:8], other[0:8]], axis=0).astype(bf16)
    out[...] = dot(hits[...], values).astype(bf16)


def spread_body(core, arrived, affine, gate, up, received, out):
    places = arrived.shape[0]
    rows = places // 2
    at, source = iota((rows, places), 0), iota((rows, places), 1)
    values = arrived[...]
    halves = []
    for half in range(2):
        takes = source == (at // SLOTS) * (2 * SLOTS) + half * SLOTS + at % SLOTS
        halves.append(dot(jnp.where(takes, 1.0, 0.0).astype(bf16), values))
    features = 2 * LANES
    mean = (
        jnp.sum(halves[0], axis=1, keepdims=True) + jnp.sum(halves[1], axis=1, keepdims=True)
    ) / features
    centred = [h - mean for h in halves]
    square = jnp.sum(centred[0] * centred[0] + centred[1] * centred[1], axis=1, keepdims=True)

    lane = iota((rows, LANES), 1)
    stats = jnp.where(lane == 0, mean, jnp.where(lane == 1, square, 0.0))
    stats = jnp.concatenate([stats, jnp.zeros((LANES - rows, LANES), f32)], axis=0).T
    means, squares = three(stats[0:1]), three(stats[1:2])

    left = []
    for half in range(2):
        lanes = slice(half * LANES, (half + 1) * LANES)
        affine_rows = affine[:, lanes]
        wide = affine_rows.astype(f32)
        gain = wide[0:1] + wide[1:2] + wide[2:3]
        left.append(jnp.concatenate([(centred[half] * gain).astype(bf16), affine_rows], axis=0))

    for mat, stat in ((0, means), (1, squares)):
        own = (gate, up)[mat][core[0]]
        total = dot(left[0], own) + dot(left[1], received[mat])
        tail = total[rows : rows + 8]
        gain_sum = tail[0:1] + tail[1:2] + tail[2:3]
        bias_sum = tail[3:4] + tail[4:5] + tail[5:6]
        parts = three(gain_sum)[0:2] + three(bias_sum)[0:2]
        for y in range(out.shape[0]):
            lanes = slice(y * LANES, (y + 1) * LANES)
            put = slice(mat * LANES, (mat + 1) * LANES)
            out[y, 0:rows, put] = total[0:rows, lanes].astype(bf16)
            out[y, rows : rows + 8, put] = by_row([p[:, lanes] for p in parts] + list(stat), LANES).astype(bf16)


def activate_body(features, parts, out):
    peers = parts.shape[0]
    rows = parts.shape[1] - 8
    tails = [parts[s, rows : rows + 8, :].astype(f32) for s in range(peers)]
    means = by_row([t[4:5, 0:LANES] + t[5:6, 0:LANES] + t[6:7, 0:LANES] for t in tails], LANES)
    squares = by_row([t[4:5, LANES:] + t[5:6, LANES:] + t[6:7, LANES:] for t in tails], LANES)
    center = jnp.sum(means, axis=0, keepdims=True) / peers
    shift = means - center
    spread = jnp.sum(squares + (features // peers) * shift * shift, axis=0, keepdims=True) / features
    scale = jnp.broadcast_to(lax.rsqrt(spread + NORM_EPSILON), (8, LANES))
    turned = jnp.concatenate([shift, scale, jnp.zeros((LANES - 16, LANES), f32)], axis=0).T

    sums = parts[0, 0:rows, :].astype(f32)
    for s in range(1, peers):
        sums = sums + parts[s, 0:rows, :].astype(f32)
    bias = tails[0][2:3] + tails[0][3:4]
    for s in range(peers):
        sums = sums + turned[0:rows, s : s + 1] * (tails[s][0:1] + tails[s][1:2])
        if s:
            bias = bias + tails[s][2:3] + tails[s][3:4]
    full = turned[0:rows, 8:9] * sums + bias
    gate, up = full[:, 0:LANES], full[:, LANES:]
    hidden = (gate / (1.0 + jnp.exp(-gate)) * up).astype(bf16)
    for s in range(peers):
        out[s] = hidden


def project_body(hidden, down, out):
    experts, tiles, rows, _ = hidden.shape
    places = out.shape[0]
    row, source = iota((places, rows), 0), iota((places, rows), 1)
    total = jnp.zeros((places, LANES), f32)
    for e in range(experts):
        wide = jnp.concatenate([hidden[e, y] for y in range(tiles)], axis=1)
        result = dot(wide, down[e]).astype(bf16)
        puts = row == (source // SLOTS) * (2 * SLOTS) + e * SLOTS + source % SLOTS
        total = total + dot(jnp.where(puts, 1.0, 0.0).astype(bf16), result)
    out[...] = total.astype(bf16)


def combine_body(returned, weights, out):
    values = returned[...]
    total = jnp.zeros(out.shape, f32)
    for part in three(weights[...]):
        total = total + lax.dot_general(
            part.astype(bf16), values, (((0,), (0,)), ((), ())), preferred_element_type=f32
        )
    out[...] = total.astype(bf16)


def on_device(
    tokens,
    norm_gain,
    norm_bias,
    group_pick,
    member_pick,
    picked_probs,
    gate_weight,
    up_weight,
    down_weight,
):
    ep = ("z", "x")
    peers = lax.axis_size(ep)
    tiles = lax.axis_size("y")
    count, width = tokens.shape
    inner = gate_weight.shape[2]
    rows = peers * SLOTS
    places = 2 * rows
    features = width * tiles * 2
    core = lax.axis_index("c")
    groups, members, probs = group_pick.T, member_pick.T, picked_probs.T

    at = core.reshape(1)
    mine, hits, weights = call(
        share_body,
        (shape((16, LANES)), shape((places, 2 * count)), shape((places, count), f32)),
        [ANY] * 6,
        scratch=[
            pltpu.VMEM((1, width), f32),
            pltpu.VMEM((1, width), f32),
            pltpu.VMEM(groups.shape, groups.dtype),
            pltpu.VMEM(members.shape, members.dtype),
            pltpu.VMEM(probs.shape, probs.dtype),
            pltpu.SemaphoreType.DMA((6,)),
        ],
    )(
        tokens,
        norm_gain.reshape(1, width),
        norm_bias.reshape(1, width),
        groups,
        members,
        probs,
    )
    sent = call(
        slice_body,
        shape((2, width, inner)),
        [SMEM, ANY, ANY],
        flops=1 << 20,
        moved=2 * width * inner * 2,
        scratch=[pltpu.SemaphoreType.DMA((2,))],
    )(at, gate_weight, up_weight)
    received = lax.ppermute(sent, "c", [(0, 1), (1, 0)])
    both = lax.all_gather(mine, "c", axis=0, tiled=False)
    outgoing, affine = call(
        pack_body, (shape((places, LANES)), shape((8, 2 * LANES))), [SMEM] + [VMEM] * 2
    )(at, both, hits)
    outgoing = outgoing.reshape(peers, 2 * SLOTS, LANES)
    arrived = lax.all_to_all(outgoing, ep, split_axis=0, concat_axis=0, tiled=True)
    arrived = arrived.reshape(places, LANES)

    parts = call(
        spread_body,
        shape((tiles, rows + 8, 2 * LANES)),
        [SMEM] + [VMEM] * 5,
        flops=2 * (rows + 8) * 2 * width * 2 * inner,
        moved=received.size * 4,
    )(at, arrived, affine, gate_weight, up_weight, received)
    parts = lax.all_to_all(parts, "y", split_axis=0, concat_axis=0, tiled=True)
    hidden = call(functools.partial(activate_body, features), shape((tiles, rows, LANES)), [VMEM])(parts)
    hidden = lax.all_to_all(hidden, "y", split_axis=0, concat_axis=0, tiled=True)
    hidden = lax.all_gather(hidden, "c", axis=0, tiled=False)
    results = call(
        project_body,
        shape((places, LANES)),
        [VMEM] * 2,
        flops=2 * rows * 2 * inner * width,
        moved=down_weight.size * 2,
    )(hidden, down_weight)
    returned = lax.all_to_all(
        results.reshape(peers, 2 * SLOTS, LANES), ep, split_axis=0, concat_axis=0, tiled=True
    ).reshape(places, LANES)
    return call(combine_body, jax.ShapeDtypeStruct((count, LANES), bf16), [VMEM] * 2)(returned, weights)


def solution(mesh):
    finer = Mesh(mesh.devices.reshape(8, 4, 8, 2), ("z", "x", "y", "c"))
    ep, tp = ("z", "x"), ("y", "c")
    placed = (
        P(ep, tp),
        P(tp),
        P(tp),
        P(ep, None),
        P(ep, None),
        P(ep, None),
        P(ep, tp, None),
        P(ep, tp, None),
        P(ep, None, tp),
    )
    return jax.shard_map(
        on_device, mesh=finer, in_specs=placed, out_specs=P(ep, tp), check_vma=False
    )
```

```python
import functools

import jax
import jax.numpy as jnp
from jax import lax
from jax.experimental import pallas as pl
from jax.experimental.pallas import tpu as pltpu
from jax.sharding import Mesh
from jax.sharding import PartitionSpec as P

f32 = jnp.float32
bf16 = jnp.bfloat16

EPG = 8
SLOTS = 2
LANES = 128
NORM_EPSILON = 1e-05

VMEM = pl.BlockSpec(memory_space=pltpu.VMEM)
SMEM = pl.BlockSpec(memory_space=pltpu.SMEM)
ANY = pl.BlockSpec(memory_space=pl.ANY)


def call(body, out_shape, in_specs, flops=0, moved=0, scratch=()):
    specs = jax.tree.map(lambda _: VMEM, out_shape)
    kernel = pl.pallas_call(
        body,
        out_shape=out_shape,
        in_specs=in_specs,
        out_specs=specs,
        scratch_shapes=scratch,
        cost_estimate=pl.CostEstimate(flops=flops, bytes_accessed=moved, transcendentals=0),
    )

    def run(*args):
        near = [
            pltpu.with_memory_space_constraint(a, pltpu.VMEM) if spec is VMEM else a
            for a, spec in zip(args, in_specs)
        ]
        return kernel(*near)

    return run


def shape(dims, dtype=bf16):
    return pltpu.VMEM(dims, dtype)


def three(value):
    high = value.astype(bf16).astype(f32)
    middle = (value - high).astype(bf16).astype(f32)
    low = (value - high - middle).astype(bf16).astype(f32)
    return high, middle, low


def iota(dims, axis):
    return lax.broadcasted_iota(jnp.int32, dims, axis)


def by_row(rows, width):
    at = iota((8, width), 0)
    out = jnp.zeros((8, width), f32)
    for i, row in enumerate(rows):
        out = jnp.where(at == i, jnp.broadcast_to(row, (8, width)), out)
    return out


def dot(a, b):
    return jnp.dot(a, b, preferred_element_type=f32)


def slots_of(groups):
    count = groups.shape[1]
    at = iota((1, count), 1)
    slots = jnp.zeros((1, count), jnp.int32)
    for j in range(count - 1):
        same = jnp.broadcast_to(groups[:, j : j + 1], (1, count)) == groups
        slots = slots + jnp.where(same & (at > j), 1, 0)
    return slots


def place_body(core, tokens, groups, members, probs, gain, bias, gate, up, out, weights, affine, *scratch):
    near_tokens, near_groups, near_members, near_probs, near_gain, near_bias, arrived = scratch
    pairs = (
        (groups, near_groups),
        (tokens, near_tokens),
        (members, near_members),
        (probs, near_probs),
        (gain, near_gain),
        (bias, near_bias),
    )
    copies = [pltpu.make_async_copy(a, b, arrived.at[i]) for i, (a, b) in enumerate(pairs)]
    for copy in copies:
        copy.start()
    for copy in copies:
        copy.wait()
    place = out.shape[0]
    per = place // 8
    chosen = near_groups[...]
    slots = slots_of(chosen)
    none = jnp.full((1, 8), -1, jnp.int32)
    pair = jnp.concatenate([chosen, none], axis=1)
    slot_pair = jnp.concatenate([slots, none], axis=1)
    row = iota((place, 16), 0)
    hit = (row // per == pair) & (row % (2 * SLOTS) == slot_pair)
    values = near_tokens[...].astype(f32)
    values = jnp.concatenate([values, jnp.zeros_like(values)], axis=0).astype(bf16)
    out[...] = dot(jnp.where(hit, 1.0, 0.0).astype(bf16), values).astype(bf16)

    likely = near_probs[...]
    shares = likely / jnp.sum(likely, axis=0, keepdims=True)
    row = iota((place, 8), 0)
    total = jnp.zeros((place, 8), f32)
    for k in range(members.shape[0]):
        member = near_members[k : k + 1, :]
        at = (chosen * (EPG // 2) + member // 2) * (2 * SLOTS) + (member % 2) * SLOTS + slots
        total = total + jnp.where(row == at, shares[k : k + 1, :], 0.0)
    weights[...] = jnp.concatenate(three(total), axis=1).astype(bf16)
    affine[...] = by_row(three(near_gain[...]) + three(near_bias[...]), LANES).astype(bf16)


def spread_body(core, arrived, affine, gate, up, kept, given):
    places = arrived.shape[0]
    rows = places // 2
    at, source = iota((rows, places), 0), iota((rows, places), 1)
    takes = source == (at // SLOTS) * (2 * SLOTS) + at % SLOTS
    values = dot(jnp.where(takes, 1.0, 0.0).astype(bf16), arrived[...])
    mean = jnp.sum(values, axis=1, keepdims=True) / LANES
    centred = values - mean
    square = jnp.sum(centred * centred, axis=1, keepdims=True)

    lane = iota((rows, LANES), 1)
    stats = jnp.where(lane == 0, mean, jnp.where(lane == 1, square, 0.0))
    stats = jnp.concatenate([stats, jnp.zeros((LANES - rows, LANES), f32)], axis=0).T

    wide = affine[...].astype(f32)
    gain = wide[0:1] + wide[1:2] + wide[2:3]
    left = jnp.concatenate([(centred * gain).astype(bf16), affine[...]], axis=0)
    none = jnp.zeros((1, LANES), f32)
    for out, expert in ((kept, core[0]), (given, 1 - core[0])):
        split = out is given
        for mat, weight in enumerate((gate, up)):
            total = dot(left, weight[expert])
            tail = total[rows : rows + 8]
            gain_sum = tail[0:1] + tail[1:2] + tail[2:3]
            bias_sum = tail[3:4] + tail[4:5] + tail[5:6]
            stat = stats[mat : mat + 1]
            put = slice(mat * LANES, (mat + 1) * LANES)
            for y in range(out.shape[0]):
                lanes = slice(y * LANES, (y + 1) * LANES)
                out[y, 0:rows, put] = total[0:rows, lanes].astype(out.dtype)
                g, b = gain_sum[:, lanes], bias_sum[:, lanes]
                parts = three(g)[0:2] + three(b)[0:2] + three(stat) if split else (g, none, b, none, stat)
                out[y, rows : rows + 8, put] = by_row(parts, LANES).astype(out.dtype)


def merge_body(width, core, kept, both, out):
    tiles, tall, wide = kept.shape
    rows = tall - 8
    peer = 1 - core[0]
    mine, theirs = kept[0, rows:tall, :], both[peer, 0, rows:tall, :].astype(f32)
    theirs = theirs[4:5] + theirs[5:6] + theirs[6:7]
    own_mean, own_square = mine[4:5, 0:LANES], mine[4:5, LANES:]
    other_mean, other_square = theirs[:, 0:LANES], theirs[:, LANES:]
    mean = (own_mean + other_mean) * 0.5
    own_shift, other_shift = own_mean - mean, other_mean - mean
    square = own_square + other_square + width * (own_shift * own_shift + other_shift * other_shift)
    stats = three(jnp.concatenate([mean, square], axis=1))
    turned = jnp.concatenate(
        [by_row([own_shift, other_shift], LANES), jnp.zeros((LANES - 8, LANES), f32)], axis=0
    ).T
    own_shift, other_shift = turned[0:rows, 0:1], turned[0:rows, 1:2]
    for y in range(tiles):
        own_tail, other_tail = kept[y, rows:tall, :], both[peer, y, rows:tall, :].astype(f32)
        own_gain, other_gain = own_tail[0:1], other_tail[0:1] + other_tail[1:2]
        bias = own_tail[2:3] + other_tail[2:3] + other_tail[3:4]
        total = kept[y, 0:rows, :] + both[peer, y, 0:rows, :].astype(f32)
        total = total + own_shift * own_gain + other_shift * other_gain
        out[y, 0:rows, :] = total.astype(bf16)
        parts = three(own_gain + other_gain)[0:2] + three(bias)[0:2] + stats
        out[y, rows:tall, :] = by_row(parts, wide).astype(bf16)


def activate_body(features, parts, out):
    peers = parts.shape[0]
    rows = parts.shape[1] - 8
    tails = [parts[s, rows : rows + 8, :].astype(f32) for s in range(peers)]
    means = by_row([t[4:5, 0:LANES] + t[5:6, 0:LANES] + t[6:7, 0:LANES] for t in tails], LANES)
    squares = by_row([t[4:5, LANES:] + t[5:6, LANES:] + t[6:7, LANES:] for t in tails], LANES)
    center = jnp.sum(means, axis=0, keepdims=True) / peers
    shift = means - center
    spread = jnp.sum(squares + (features // peers) * shift * shift, axis=0, keepdims=True) / features
    scale = jnp.broadcast_to(lax.rsqrt(spread + NORM_EPSILON), (8, LANES))
    turned = jnp.concatenate([shift, scale, jnp.zeros((LANES - 16, LANES), f32)], axis=0).T

    sums = parts[0, 0:rows, :].astype(f32)
    for s in range(1, peers):
        sums = sums + parts[s, 0:rows, :].astype(f32)
    bias = tails[0][2:3] + tails[0][3:4]
    for s in range(peers):
        sums = sums + turned[0:rows, s : s + 1] * (tails[s][0:1] + tails[s][1:2])
        if s:
            bias = bias + tails[s][2:3] + tails[s][3:4]
    full = turned[0:rows, 8:9] * sums + bias
    gate, up = full[:, 0:LANES], full[:, LANES:]
    hidden = (gate / (1.0 + jnp.exp(-gate)) * up).astype(bf16)
    for s in range(peers):
        out[s] = hidden


def project_body(hidden, down, out):
    experts, tiles, rows, width = hidden.shape
    places = out.shape[0]
    row, source = iota((places, rows), 0), iota((places, rows), 1)
    total = jnp.zeros((places, LANES), f32)
    for e in range(experts):
        wide = jnp.concatenate([hidden[e, y] for y in range(tiles)], axis=1)
        result = dot(wide, down[e]).astype(bf16)
        puts = row == (source // SLOTS) * (2 * SLOTS) + e * SLOTS + source % SLOTS
        total = total + dot(jnp.where(puts, 1.0, 0.0).astype(bf16), result)
    out[...] = total.astype(bf16)


def combine_body(returned, weights, out):
    count = out.shape[0]
    total = lax.dot_general(
        weights[...], returned[...], (((0,), (0,)), ((), ())), preferred_element_type=f32
    )
    total = total[0:count] + total[count : 2 * count] + total[2 * count :]
    out[...] = total.astype(bf16)


def on_device(
    tokens,
    norm_gain,
    norm_bias,
    group_pick,
    member_pick,
    picked_probs,
    gate_weight,
    up_weight,
    down_weight,
):
    ep = ("z", "x")
    peers = lax.axis_size(ep)
    tiles = lax.axis_size("y")
    count, width = tokens.shape
    inner = gate_weight.shape[2]
    rows = peers * SLOTS
    places = 2 * rows
    features = width * tiles * 2
    core = lax.axis_index("c")
    groups, members, probs = group_pick.T, member_pick.T, picked_probs.T

    at = core.reshape(1)
    outgoing, weights, affine = call(
        place_body,
        (shape((places, LANES)), shape((places, 3 * count)), shape((8, LANES))),
        [SMEM] + [ANY] * 8,
        scratch=[
            pltpu.VMEM(tokens.shape, tokens.dtype),
            pltpu.VMEM(groups.shape, groups.dtype),
            pltpu.VMEM(members.shape, members.dtype),
            pltpu.VMEM(probs.shape, probs.dtype),
            pltpu.VMEM((1, width), f32),
            pltpu.VMEM((1, width), f32),
            pltpu.SemaphoreType.DMA((6,)),
        ],
    )(
        at,
        tokens,
        groups,
        members,
        probs,
        norm_gain.reshape(1, width),
        norm_bias.reshape(1, width),
        gate_weight,
        up_weight,
    )
    arrived = lax.all_to_all(
        outgoing.reshape(peers, 2 * SLOTS, LANES), ep, split_axis=0, concat_axis=0, tiled=True
    ).reshape(places, LANES)

    whole = (tiles, rows + 8, 2 * LANES)
    kept, given = call(
        spread_body,
        (shape(whole, f32), shape(whole)),
        [SMEM] + [VMEM] * 4,
        flops=2 * (rows + 8) * width * 4 * inner,
        moved=gate_weight.size * 4,
    )(at, arrived, affine, gate_weight, up_weight)
    both = lax.all_gather(given, "c", axis=0, tiled=False)
    parts = call(functools.partial(merge_body, width), shape(whole), [SMEM] + [VMEM] * 2)(at, kept, both)
    parts = lax.all_to_all(parts, "y", split_axis=0, concat_axis=0, tiled=True)
    hidden = call(functools.partial(activate_body, features), shape((tiles, rows, LANES)), [VMEM])(parts)
    hidden = lax.all_to_all(hidden, "y", split_axis=0, concat_axis=0, tiled=True)
    hidden = lax.all_gather(hidden, "c", axis=0, tiled=False)
    results = call(
        project_body,
        shape((places, LANES)),
        [VMEM] * 2,
        flops=2 * rows * 2 * inner * width,
        moved=down_weight.size * 2,
    )(hidden, down_weight)
    returned = lax.all_to_all(
        results.reshape(peers, 2 * SLOTS, LANES), ep, split_axis=0, concat_axis=0, tiled=True
    ).reshape(places, LANES)
    return call(combine_body, jax.ShapeDtypeStruct((count, LANES), bf16), [VMEM] * 2)(returned, weights)


def solution(mesh):
    finer = Mesh(mesh.devices.reshape(8, 4, 8, 2), ("z", "x", "y", "c"))
    ep, tp = ("z", "x"), ("y", "c")
    placed = (
        P(ep, tp),
        P(tp),
        P(tp),
        P(ep, None),
        P(ep, None),
        P(ep, None),
        P(ep, tp, None),
        P(ep, tp, None),
        P(ep, None, tp),
    )
    return jax.shard_map(
        on_device, mesh=finer, in_specs=placed, out_specs=P(ep, tp), check_vma=False
    )
```

```python
import functools

import jax
import jax.numpy as jnp
from jax import lax
from jax.experimental import pallas as pl
from jax.experimental.pallas import tpu as pltpu
from jax.sharding import Mesh
from jax.sharding import PartitionSpec as P

f32 = jnp.float32
bf16 = jnp.bfloat16

EPG = 8
SLOTS = 2
LANES = 128
NORM_EPSILON = 1e-05

VMEM = pl.BlockSpec(memory_space=pltpu.VMEM)
SMEM = pl.BlockSpec(memory_space=pltpu.SMEM)
ANY = pl.BlockSpec(memory_space=pl.ANY)


def call(body, out_shape, in_specs, flops=0, moved=0, scratch=()):
    specs = jax.tree.map(lambda _: VMEM, out_shape)
    kernel = pl.pallas_call(
        body,
        out_shape=out_shape,
        in_specs=in_specs,
        out_specs=specs,
        scratch_shapes=scratch,
        cost_estimate=pl.CostEstimate(flops=flops, bytes_accessed=moved, transcendentals=0),
    )

    def run(*args):
        near = [
            pltpu.with_memory_space_constraint(a, pltpu.VMEM) if spec is VMEM else a
            for a, spec in zip(args, in_specs)
        ]
        return kernel(*near)

    return run


def shape(dims, dtype=bf16):
    return pltpu.VMEM(dims, dtype)


def three(value):
    high = value.astype(bf16).astype(f32)
    middle = (value - high).astype(bf16).astype(f32)
    low = (value - high - middle).astype(bf16).astype(f32)
    return high, middle, low


def iota(dims, axis):
    return lax.broadcasted_iota(jnp.int32, dims, axis)


def by_row(rows, width):
    at = iota((8, width), 0)
    out = jnp.zeros((8, width), f32)
    for i, row in enumerate(rows):
        out = jnp.where(at == i, jnp.broadcast_to(row, (8, width)), out)
    return out


def dot(a, b):
    return jnp.dot(a, b, preferred_element_type=f32)


def slots_of(groups):
    count = groups.shape[1]
    at = iota((1, count), 1)
    slots = jnp.zeros((1, count), jnp.int32)
    for j in range(count - 1):
        same = jnp.broadcast_to(groups[:, j : j + 1], (1, count)) == groups
        slots = slots + jnp.where(same & (at > j), 1, 0)
    return slots


def place_body(core, tokens, groups, members, probs, gain, bias, gate, up, out, weights, affine, *scratch):
    near_tokens, near_groups, near_members, near_probs, near_gain, near_bias, arrived = scratch
    pairs = (
        (groups, near_groups),
        (tokens, near_tokens),
        (members, near_members),
        (probs, near_probs),
        (gain, near_gain),
        (bias, near_bias),
    )
    copies = [pltpu.make_async_copy(a, b, arrived.at[i]) for i, (a, b) in enumerate(pairs)]
    for copy in copies:
        copy.start()
    for copy in copies:
        copy.wait()
    place = out.shape[0]
    per = place // 8
    chosen = near_groups[...]
    slots = slots_of(chosen)
    none = jnp.full((1, 8), -1, jnp.int32)
    pair = jnp.concatenate([chosen, none], axis=1)
    slot_pair = jnp.concatenate([slots, none], axis=1)
    row = iota((place, 16), 0)
    hit = (row // per == pair) & (row % SLOTS == slot_pair)
    values = near_tokens[...].astype(f32)
    values = jnp.concatenate([values, jnp.zeros_like(values)], axis=0).astype(bf16)
    out[...] = dot(jnp.where(hit, 1.0, 0.0).astype(bf16), values).astype(bf16)

    likely = near_probs[...]
    shares = likely / jnp.sum(likely, axis=0, keepdims=True)
    row = iota((2 * place, 8), 0)
    total = jnp.zeros((2 * place, 8), f32)
    for k in range(members.shape[0]):
        member = near_members[k : k + 1, :]
        at = (chosen * (EPG // 2) + member // 2) * (2 * SLOTS) + (member % 2) * SLOTS + slots
        total = total + jnp.where(row == at, shares[k : k + 1, :], 0.0)
    weights[...] = jnp.concatenate(three(total), axis=1).astype(bf16)
    affine[...] = by_row(three(near_gain[...]) + three(near_bias[...]), LANES).astype(bf16)


def spread_body(core, arrived, affine, gate, up, kept, given):
    rows = arrived.shape[0]
    values = arrived[...].astype(f32)
    mean = jnp.sum(values, axis=1, keepdims=True) / LANES
    centred = values - mean
    square = jnp.sum(centred * centred, axis=1, keepdims=True)

    lane = iota((rows, LANES), 1)
    stats = jnp.where(lane == 0, mean, jnp.where(lane == 1, square, 0.0))
    stats = jnp.concatenate([stats, jnp.zeros((LANES - rows, LANES), f32)], axis=0).T

    wide = affine[...].astype(f32)
    gain = wide[0:1] + wide[1:2] + wide[2:3]
    left = jnp.concatenate([(centred * gain).astype(bf16), affine[...]], axis=0)
    none = jnp.zeros((1, LANES), f32)
    for out, expert in ((kept, core[0]), (given, 1 - core[0])):
        split = out is given
        for mat, weight in enumerate((gate, up)):
            total = dot(left, weight[expert])
            tail = total[rows : rows + 8]
            gain_sum = tail[0:1] + tail[1:2] + tail[2:3]
            bias_sum = tail[3:4] + tail[4:5] + tail[5:6]
            stat = stats[mat : mat + 1]
            put = slice(mat * LANES, (mat + 1) * LANES)
            for y in range(out.shape[0]):
                lanes = slice(y * LANES, (y + 1) * LANES)
                out[y, 0:rows, put] = total[0:rows, lanes].astype(out.dtype)
                g, b = gain_sum[:, lanes], bias_sum[:, lanes]
                parts = three(g)[0:2] + three(b)[0:2] + three(stat) if split else (g, none, b, none, stat)
                out[y, rows : rows + 8, put] = by_row(parts, LANES).astype(out.dtype)


def merge_body(width, core, kept, both, out):
    tiles, tall, wide = kept.shape
    rows = tall - 8
    peer = 1 - core[0]
    mine, theirs = kept[0, rows:tall, :], both[peer, 0, rows:tall, :].astype(f32)
    theirs = theirs[4:5] + theirs[5:6] + theirs[6:7]
    own_mean, own_square = mine[4:5, 0:LANES], mine[4:5, LANES:]
    other_mean, other_square = theirs[:, 0:LANES], theirs[:, LANES:]
    mean = (own_mean + other_mean) * 0.5
    own_shift, other_shift = own_mean - mean, other_mean - mean
    square = own_square + other_square + width * (own_shift * own_shift + other_shift * other_shift)
    stats = three(jnp.concatenate([mean, square], axis=1))
    turned = jnp.concatenate(
        [by_row([own_shift, other_shift], LANES), jnp.zeros((LANES - 8, LANES), f32)], axis=0
    ).T
    own_shift, other_shift = turned[0:rows, 0:1], turned[0:rows, 1:2]
    for y in range(tiles):
        own_tail, other_tail = kept[y, rows:tall, :], both[peer, y, rows:tall, :].astype(f32)
        own_gain, other_gain = own_tail[0:1], other_tail[0:1] + other_tail[1:2]
        bias = own_tail[2:3] + other_tail[2:3] + other_tail[3:4]
        total = kept[y, 0:rows, :] + both[peer, y, 0:rows, :].astype(f32)
        total = total + own_shift * own_gain + other_shift * other_gain
        out[y, 0:rows, :] = total.astype(bf16)
        parts = three(own_gain + other_gain)[0:2] + three(bias)[0:2] + stats
        out[y, rows:tall, :] = by_row(parts, wide).astype(bf16)


def activate_body(features, parts, out):
    peers = parts.shape[0]
    rows = parts.shape[1] - 8
    tails = [parts[s, rows : rows + 8, :].astype(f32) for s in range(peers)]
    means = by_row([t[4:5, 0:LANES] + t[5:6, 0:LANES] + t[6:7, 0:LANES] for t in tails], LANES)
    squares = by_row([t[4:5, LANES:] + t[5:6, LANES:] + t[6:7, LANES:] for t in tails], LANES)
    center = jnp.sum(means, axis=0, keepdims=True) / peers
    shift = means - center
    spread = jnp.sum(squares + (features // peers) * shift * shift, axis=0, keepdims=True) / features
    scale = jnp.broadcast_to(lax.rsqrt(spread + NORM_EPSILON), (8, LANES))
    turned = jnp.concatenate([shift, scale, jnp.zeros((LANES - 16, LANES), f32)], axis=0).T

    sums = parts[0, 0:rows, :].astype(f32)
    for s in range(1, peers):
        sums = sums + parts[s, 0:rows, :].astype(f32)
    bias = tails[0][2:3] + tails[0][3:4]
    for s in range(peers):
        sums = sums + turned[0:rows, s : s + 1] * (tails[s][0:1] + tails[s][1:2])
        if s:
            bias = bias + tails[s][2:3] + tails[s][3:4]
    full = turned[0:rows, 8:9] * sums + bias
    gate, up = full[:, 0:LANES], full[:, LANES:]
    hidden = (gate / (1.0 + jnp.exp(-gate)) * up).astype(bf16)
    for s in range(peers):
        out[s] = hidden


def project_body(hidden, down, out):
    experts, tiles, rows, width = hidden.shape
    places = out.shape[0]
    row, source = iota((places, rows), 0), iota((places, rows), 1)
    total = jnp.zeros((places, LANES), f32)
    for e in range(experts):
        wide = jnp.concatenate([hidden[e, y] for y in range(tiles)], axis=1)
        result = dot(wide, down[e]).astype(bf16)
        puts = row == (source // SLOTS) * (2 * SLOTS) + e * SLOTS + source % SLOTS
        total = total + dot(jnp.where(puts, 1.0, 0.0).astype(bf16), result)
    out[...] = total.astype(bf16)


def combine_body(returned, weights, out):
    count = out.shape[0]
    total = lax.dot_general(
        weights[...], returned[...], (((0,), (0,)), ((), ())), preferred_element_type=f32
    )
    total = total[0:count] + total[count : 2 * count] + total[2 * count :]
    out[...] = total.astype(bf16)


def on_device(
    tokens,
    norm_gain,
    norm_bias,
    group_pick,
    member_pick,
    picked_probs,
    gate_weight,
    up_weight,
    down_weight,
):
    ep = ("z", "x")
    peers = lax.axis_size(ep)
    tiles = lax.axis_size("y")
    count, width = tokens.shape
    inner = gate_weight.shape[2]
    rows = peers * SLOTS
    places = 2 * rows
    features = width * tiles * 2
    core = lax.axis_index("c")
    groups, members, probs = group_pick.T, member_pick.T, picked_probs.T

    at = core.reshape(1)
    outgoing, weights, affine = call(
        place_body,
        (shape((rows, LANES)), shape((places, 3 * count)), shape((8, LANES))),
        [SMEM] + [ANY] * 8,
        scratch=[
            pltpu.VMEM(tokens.shape, tokens.dtype),
            pltpu.VMEM(groups.shape, groups.dtype),
            pltpu.VMEM(members.shape, members.dtype),
            pltpu.VMEM(probs.shape, probs.dtype),
            pltpu.VMEM((1, width), f32),
            pltpu.VMEM((1, width), f32),
            pltpu.SemaphoreType.DMA((6,)),
        ],
    )(
        at,
        tokens,
        groups,
        members,
        probs,
        norm_gain.reshape(1, width),
        norm_bias.reshape(1, width),
        gate_weight,
        up_weight,
    )
    arrived = lax.all_to_all(
        outgoing.reshape(peers, SLOTS, LANES), ep, split_axis=0, concat_axis=0, tiled=True
    ).reshape(rows, LANES)

    whole = (tiles, rows + 8, 2 * LANES)
    kept, given = call(
        spread_body,
        (shape(whole, f32), shape(whole)),
        [SMEM] + [VMEM] * 4,
        flops=2 * (rows + 8) * width * 4 * inner,
        moved=gate_weight.size * 4,
    )(at, arrived, affine, gate_weight, up_weight)
    both = lax.all_gather(given, "c", axis=0, tiled=False)
    parts = call(functools.partial(merge_body, width), shape(whole), [SMEM] + [VMEM] * 2)(at, kept, both)
    parts = lax.all_to_all(parts, "y", split_axis=0, concat_axis=0, tiled=True)
    hidden = call(functools.partial(activate_body, features), shape((tiles, rows, LANES)), [VMEM])(parts)
    hidden = lax.all_to_all(hidden, "y", split_axis=0, concat_axis=0, tiled=True)
    hidden = lax.all_gather(hidden, "c", axis=0, tiled=False)
    results = call(
        project_body,
        shape((places, LANES)),
        [VMEM] * 2,
        flops=2 * rows * 2 * inner * width,
        moved=down_weight.size * 2,
    )(hidden, down_weight)
    returned = lax.all_to_all(
        results.reshape(peers, 2 * SLOTS, LANES), ep, split_axis=0, concat_axis=0, tiled=True
    ).reshape(places, LANES)
    return call(combine_body, jax.ShapeDtypeStruct((count, LANES), bf16), [VMEM] * 2)(returned, weights)


def solution(mesh):
    finer = Mesh(mesh.devices.reshape(8, 4, 8, 2), ("z", "x", "y", "c"))
    ep, tp = ("z", "x"), ("y", "c")
    placed = (
        P(ep, tp),
        P(tp),
        P(tp),
        P(ep, None),
        P(ep, None),
        P(ep, None),
        P(ep, tp, None),
        P(ep, tp, None),
        P(ep, None, tp),
    )
    return jax.shard_map(
        on_device, mesh=finer, in_specs=placed, out_specs=P(ep, tp), check_vma=False
    )
```

```python
import functools

import jax
import jax.numpy as jnp
from jax import lax
from jax.experimental import pallas as pl
from jax.experimental.pallas import tpu as pltpu
from jax.sharding import Mesh
from jax.sharding import PartitionSpec as P

f32 = jnp.float32
bf16 = jnp.bfloat16

EPG = 8
SLOTS = 2
LANES = 128
SUMS_Y = [4, 3, 5, 2, 6, 1, 7, 0]
ROWS_Y = [4, 3, 5, 2, 6, 1, 7, 0]
OUT_Z, OUT_X = [4, 3, 5, 2, 6, 1, 7, 0], [2, 1, 3, 0]
BACK_Z, BACK_X = [4, 3, 5, 2, 6, 1, 7, 0], [2, 1, 3, 0]
NORM_EPSILON = 1e-05

VMEM = pl.BlockSpec(memory_space=pltpu.VMEM)
SMEM = pl.BlockSpec(memory_space=pltpu.SMEM)
ANY = pl.BlockSpec(memory_space=pl.ANY)


def call(body, out_shape, in_specs, flops=0, moved=0, scratch=()):
    specs = jax.tree.map(lambda _: VMEM, out_shape)
    kernel = pl.pallas_call(
        body,
        out_shape=out_shape,
        in_specs=in_specs,
        out_specs=specs,
        scratch_shapes=scratch,
        cost_estimate=pl.CostEstimate(flops=flops, bytes_accessed=moved, transcendentals=0),
    )

    def run(*args):
        near = [
            pltpu.with_memory_space_constraint(a, pltpu.VMEM) if spec is VMEM else a
            for a, spec in zip(args, in_specs)
        ]
        return kernel(*near)

    return run


def shape(dims, dtype=bf16):
    return pltpu.VMEM(dims, dtype)


def three(value):
    high = value.astype(bf16).astype(f32)
    middle = (value - high).astype(bf16).astype(f32)
    low = (value - high - middle).astype(bf16).astype(f32)
    return high, middle, low


def iota(dims, axis):
    return lax.broadcasted_iota(jnp.int32, dims, axis)


def place_in(order, values):
    at = jnp.zeros_like(values)
    for i, value in enumerate(order):
        at = jnp.where(values == value, i, at)
    return at


def ends(order_z, order_x):
    return [z * len(order_x) + x for z in order_z for x in order_x]


def by_row(rows, width):
    at = iota((8, width), 0)
    out = jnp.zeros((8, width), f32)
    for i, row in enumerate(rows):
        out = jnp.where(at == i, jnp.broadcast_to(row, (8, width)), out)
    return out


def dot(a, b):
    return jnp.dot(a, b, preferred_element_type=f32)


def slots_of(groups):
    count = groups.shape[1]
    at = iota((1, count), 1)
    slots = jnp.zeros((1, count), jnp.int32)
    for j in range(count - 1):
        same = jnp.broadcast_to(groups[:, j : j + 1], (1, count)) == groups
        slots = slots + jnp.where(same & (at > j), 1, 0)
    return slots


def place_body(core, tokens, groups, members, probs, gain, bias, gate, up, out, weights, affine, *scratch):
    near_tokens, near_groups, near_members, near_probs, near_gain, near_bias, arrived = scratch
    pairs = (
        (groups, near_groups),
        (tokens, near_tokens),
        (members, near_members),
        (probs, near_probs),
        (gain, near_gain),
        (bias, near_bias),
    )
    copies = [pltpu.make_async_copy(a, b, arrived.at[i]) for i, (a, b) in enumerate(pairs)]
    for copy in copies:
        copy.start()
    for copy in copies:
        copy.wait()
    place = out.shape[0]
    per = place // 8
    chosen = near_groups[...]
    slots = slots_of(chosen)
    none = jnp.full((1, 8), -1, jnp.int32)
    pair = jnp.concatenate([place_in(OUT_Z, chosen), none], axis=1)
    slot_pair = jnp.concatenate([slots, none], axis=1)
    row = iota((place, 16), 0)
    hit = (row // per == pair) & (row % SLOTS == slot_pair)
    values = near_tokens[...].astype(f32)
    values = jnp.concatenate([values, jnp.zeros_like(values)], axis=0).astype(bf16)
    out[...] = dot(jnp.where(hit, 1.0, 0.0).astype(bf16), values).astype(bf16)

    likely = near_probs[...]
    shares = likely / jnp.sum(likely, axis=0, keepdims=True)
    row = iota((2 * place, 8), 0)
    total = jnp.zeros((2 * place, 8), f32)
    for k in range(members.shape[0]):
        member = near_members[k : k + 1, :]
        at = (place_in(BACK_Z, chosen) * (EPG // 2) + place_in(BACK_X, member // 2)) * (2 * SLOTS) + (member % 2) * SLOTS + slots
        total = total + jnp.where(row == at, shares[k : k + 1, :], 0.0)
    weights[...] = jnp.concatenate(three(total), axis=1).astype(bf16)
    affine[...] = by_row(three(near_gain[...]) + three(near_bias[...]), LANES).astype(bf16)


def spread_body(core, arrived, affine, gate, up, kept, given):
    rows = arrived.shape[0]
    values = arrived[...].astype(f32)
    mean = jnp.sum(values, axis=1, keepdims=True) / LANES
    centred = values - mean
    square = jnp.sum(centred * centred, axis=1, keepdims=True)

    lane = iota((rows, LANES), 1)
    stats = jnp.where(lane == 0, mean, jnp.where(lane == 1, square, 0.0))
    stats = jnp.concatenate([stats, jnp.zeros((LANES - rows, LANES), f32)], axis=0).T

    wide = affine[...].astype(f32)
    gain = wide[0:1] + wide[1:2] + wide[2:3]
    left = jnp.concatenate([(centred * gain).astype(bf16), affine[...]], axis=0)
    none = jnp.zeros((1, LANES), f32)
    for out, expert in ((kept, core[0]), (given, 1 - core[0])):
        split = out is given
        for mat, weight in enumerate((gate, up)):
            total = dot(left, weight[expert])
            tail = total[rows : rows + 8]
            gain_sum = tail[0:1] + tail[1:2] + tail[2:3]
            bias_sum = tail[3:4] + tail[4:5] + tail[5:6]
            stat = stats[mat : mat + 1]
            put = slice(mat * LANES, (mat + 1) * LANES)
            for y in range(out.shape[0]):
                lanes = slice(y * LANES, (y + 1) * LANES)
                out[y, 0:rows, put] = total[0:rows, lanes].astype(out.dtype)
                g, b = gain_sum[:, lanes], bias_sum[:, lanes]
                parts = three(g)[0:2] + three(b)[0:2] + three(stat) if split else (g, none, b, none, stat)
                out[y, rows : rows + 8, put] = by_row(parts, LANES).astype(out.dtype)


def merge_body(width, core, kept, both, out):
    tiles, tall, wide = kept.shape
    rows = tall - 8
    peer = 1 - core[0]
    mine, theirs = kept[0, rows:tall, :], both[peer, 0, rows:tall, :].astype(f32)
    theirs = theirs[4:5] + theirs[5:6] + theirs[6:7]
    own_mean, own_square = mine[4:5, 0:LANES], mine[4:5, LANES:]
    other_mean, other_square = theirs[:, 0:LANES], theirs[:, LANES:]
    mean = (own_mean + other_mean) * 0.5
    own_shift, other_shift = own_mean - mean, other_mean - mean
    square = own_square + other_square + width * (own_shift * own_shift + other_shift * other_shift)
    stats = three(jnp.concatenate([mean, square], axis=1))
    turned = jnp.concatenate(
        [by_row([own_shift, other_shift], LANES), jnp.zeros((LANES - 8, LANES), f32)], axis=0
    ).T
    own_shift, other_shift = turned[0:rows, 0:1], turned[0:rows, 1:2]
    for y in range(tiles):
        own_tail, other_tail = kept[y, rows:tall, :], both[peer, y, rows:tall, :].astype(f32)
        own_gain, other_gain = own_tail[0:1], other_tail[0:1] + other_tail[1:2]
        bias = own_tail[2:3] + other_tail[2:3] + other_tail[3:4]
        total = kept[y, 0:rows, :] + both[peer, y, 0:rows, :].astype(f32)
        total = total + own_shift * own_gain + other_shift * other_gain
        out[y, 0:rows, :] = total.astype(bf16)
        parts = three(own_gain + other_gain)[0:2] + three(bias)[0:2] + stats
        out[y, rows:tall, :] = by_row(parts, wide).astype(bf16)


def activate_body(features, parts, out):
    peers = parts.shape[0]
    rows = parts.shape[1] - 8
    tails = [parts[s, rows : rows + 8, :].astype(f32) for s in range(peers)]
    means = by_row([t[4:5, 0:LANES] + t[5:6, 0:LANES] + t[6:7, 0:LANES] for t in tails], LANES)
    squares = by_row([t[4:5, LANES:] + t[5:6, LANES:] + t[6:7, LANES:] for t in tails], LANES)
    center = jnp.sum(means, axis=0, keepdims=True) / peers
    shift = means - center
    spread = jnp.sum(squares + (features // peers) * shift * shift, axis=0, keepdims=True) / features
    scale = jnp.broadcast_to(lax.rsqrt(spread + NORM_EPSILON), (8, LANES))
    turned = jnp.concatenate([shift, scale, jnp.zeros((LANES - 16, LANES), f32)], axis=0).T

    sums = parts[0, 0:rows, :].astype(f32)
    for s in range(1, peers):
        sums = sums + parts[s, 0:rows, :].astype(f32)
    bias = tails[0][2:3] + tails[0][3:4]
    for s in range(peers):
        sums = sums + turned[0:rows, s : s + 1] * (tails[s][0:1] + tails[s][1:2])
        if s:
            bias = bias + tails[s][2:3] + tails[s][3:4]
    full = turned[0:rows, 8:9] * sums + bias
    gate, up = full[:, 0:LANES], full[:, LANES:]
    hidden = (gate / (1.0 + jnp.exp(-gate)) * up).astype(bf16)
    for s in range(peers):
        out[s] = hidden


def project_body(hidden, down, out):
    experts, tiles, rows, width = hidden.shape
    places = out.shape[0]
    row, source = iota((places, rows), 0), iota((places, rows), 1)
    total = jnp.zeros((places, LANES), f32)
    for e in range(experts):
        wide = jnp.concatenate([hidden[e, ROWS_Y.index(y)] for y in SUMS_Y], axis=1)
        result = dot(wide, down[e]).astype(bf16)
        puts = row == (source // SLOTS) * (2 * SLOTS) + e * SLOTS + source % SLOTS
        total = total + dot(jnp.where(puts, 1.0, 0.0).astype(bf16), result)
    out[...] = total.astype(bf16)


def combine_body(returned, weights, out):
    count = out.shape[0]
    total = lax.dot_general(
        weights[...], returned[...], (((0,), (0,)), ((), ())), preferred_element_type=f32
    )
    total = total[0:count] + total[count : 2 * count] + total[2 * count :]
    out[...] = total.astype(bf16)


def on_device(
    tokens,
    norm_gain,
    norm_bias,
    group_pick,
    member_pick,
    picked_probs,
    gate_weight,
    up_weight,
    down_weight,
):
    ep = "e"
    peers = lax.axis_size(ep)
    tiles = lax.axis_size("y")
    count, width = tokens.shape
    inner = gate_weight.shape[2]
    rows = peers * SLOTS
    places = 2 * rows
    features = width * tiles * 2
    core = lax.axis_index("c")
    groups, members, probs = group_pick.T, member_pick.T, picked_probs.T

    at = core.reshape(1)
    outgoing, weights, affine = call(
        place_body,
        (shape((rows, LANES)), shape((places, 3 * count)), shape((8, LANES))),
        [SMEM] + [ANY] * 8,
        scratch=[
            pltpu.VMEM(tokens.shape, tokens.dtype),
            pltpu.VMEM(groups.shape, groups.dtype),
            pltpu.VMEM(members.shape, members.dtype),
            pltpu.VMEM(probs.shape, probs.dtype),
            pltpu.VMEM((1, width), f32),
            pltpu.VMEM((1, width), f32),
            pltpu.SemaphoreType.DMA((6,)),
        ],
    )(
        at,
        tokens,
        groups,
        members,
        probs,
        norm_gain.reshape(1, width),
        norm_bias.reshape(1, width),
        gate_weight,
        up_weight,
    )
    arrived = lax.all_to_all(
        outgoing.reshape(peers, SLOTS, LANES), ep, split_axis=0, concat_axis=0, tiled=True, axis_index_groups=[ends(OUT_Z, OUT_X)]
    ).reshape(rows, LANES)

    whole = (tiles, rows + 8, 2 * LANES)
    kept, given = call(
        spread_body,
        (shape(whole, f32), shape(whole)),
        [SMEM] + [VMEM] * 4,
        flops=2 * (rows + 8) * width * 4 * inner,
        moved=gate_weight.size * 4,
    )(at, arrived, affine, gate_weight, up_weight)
    both = lax.all_gather(given, "c", axis=0, tiled=False)
    parts = call(functools.partial(merge_body, width), shape(whole), [SMEM] + [VMEM] * 2)(at, kept, both)
    parts = lax.all_to_all(
        parts, "y", split_axis=0, concat_axis=0, tiled=True, axis_index_groups=[SUMS_Y]
    )
    hidden = call(functools.partial(activate_body, features), shape((tiles, rows, LANES)), [VMEM])(parts)
    hidden = lax.all_to_all(
        hidden, "y", split_axis=0, concat_axis=0, tiled=True, axis_index_groups=[ROWS_Y]
    )
    hidden = lax.all_gather(hidden, "c", axis=0, tiled=False)
    results = call(
        project_body,
        shape((places, LANES)),
        [VMEM] * 2,
        flops=2 * rows * 2 * inner * width,
        moved=down_weight.size * 2,
    )(hidden, down_weight)
    returned = lax.all_to_all(
        results.reshape(peers, 2 * SLOTS, LANES), ep, split_axis=0, concat_axis=0, tiled=True, axis_index_groups=[ends(BACK_Z, BACK_X)]
    ).reshape(places, LANES)
    return call(combine_body, jax.ShapeDtypeStruct((count, LANES), bf16), [VMEM] * 2)(returned, weights)


def solution(mesh):
    finer = Mesh(mesh.devices.reshape(32, 8, 2), ("e", "y", "c"))
    ep, tp = "e", ("y", "c")
    placed = (
        P(ep, tp),
        P(tp),
        P(tp),
        P(ep, None),
        P(ep, None),
        P(ep, None),
        P(ep, tp, None),
        P(ep, tp, None),
        P(ep, None, tp),
    )
    return jax.shard_map(
        on_device, mesh=finer, in_specs=placed, out_specs=P(ep, tp), check_vma=False
    )
```

```python
import functools

import jax
import jax.numpy as jnp
from jax import lax
from jax.experimental import pallas as pl
from jax.experimental.pallas import tpu as pltpu
from jax.sharding import Mesh
from jax.sharding import PartitionSpec as P

f32 = jnp.float32
bf16 = jnp.bfloat16

EPG = 8
SLOTS = 2
LANES = 128
SUMS_Y = [4, 3, 5, 2, 6, 1, 7, 0]
ROWS_Y = [4, 3, 5, 2, 6, 1, 7, 0]
OUT_Z, OUT_X = [4, 3, 5, 2, 6, 1, 7, 0], [2, 1, 3, 0]
BACK_Z, BACK_X = [4, 3, 5, 2, 6, 1, 7, 0], [2, 1, 3, 0]
NORM_EPSILON = 1e-05

VMEM = pl.BlockSpec(memory_space=pltpu.VMEM)
SMEM = pl.BlockSpec(memory_space=pltpu.SMEM)
ANY = pl.BlockSpec(memory_space=pl.ANY)


def call(body, out_shape, in_specs, flops=0, moved=0, scratch=()):
    specs = jax.tree.map(lambda _: VMEM, out_shape)
    kernel = pl.pallas_call(
        body,
        out_shape=out_shape,
        in_specs=in_specs,
        out_specs=specs,
        scratch_shapes=scratch,
        cost_estimate=pl.CostEstimate(flops=flops, bytes_accessed=moved, transcendentals=0),
    )

    def run(*args):
        near = [
            pltpu.with_memory_space_constraint(a, pltpu.VMEM) if spec is VMEM else a
            for a, spec in zip(args, in_specs)
        ]
        return kernel(*near)

    return run


def shape(dims, dtype=bf16):
    return pltpu.VMEM(dims, dtype)


def three(value):
    high = value.astype(bf16).astype(f32)
    middle = (value - high).astype(bf16).astype(f32)
    low = (value - high - middle).astype(bf16).astype(f32)
    return high, middle, low


def iota(dims, axis):
    return lax.broadcasted_iota(jnp.int32, dims, axis)


def place_in(order, values):
    at = jnp.zeros_like(values)
    for i, value in enumerate(order):
        at = jnp.where(values == value, i, at)
    return at


def ends(order_z, order_x):
    return [z * len(order_x) + x for z in order_z for x in order_x]


def by_row(rows, width):
    at = iota((8, width), 0)
    out = jnp.zeros((8, width), f32)
    for i, row in enumerate(rows):
        out = jnp.where(at == i, jnp.broadcast_to(row, (8, width)), out)
    return out


def dot(a, b):
    return jnp.dot(a, b, preferred_element_type=f32)


def slots_of(groups):
    count = groups.shape[1]
    at = iota((1, count), 1)
    slots = jnp.zeros((1, count), jnp.int32)
    for j in range(count - 1):
        same = jnp.broadcast_to(groups[:, j : j + 1], (1, count)) == groups
        slots = slots + jnp.where(same & (at > j), 1, 0)
    return slots


def place_body(core, tokens, groups, members, probs, gain, bias, gate, up, out, weights, affine, *scratch):
    near_tokens, near_groups, near_members, near_probs, near_gain, near_bias, arrived = scratch
    pairs = (
        (groups, near_groups),
        (tokens, near_tokens),
        (members, near_members),
        (probs, near_probs),
        (gain, near_gain),
        (bias, near_bias),
    )
    copies = [pltpu.make_async_copy(a, b, arrived.at[i]) for i, (a, b) in enumerate(pairs)]
    for copy in copies:
        copy.start()
    for copy in copies:
        copy.wait()
    place = out.shape[0]
    per = place // 8
    chosen = near_groups[...]
    slots = slots_of(chosen)
    none = jnp.full((1, 8), -1, jnp.int32)
    pair = jnp.concatenate([place_in(OUT_Z, chosen), none], axis=1)
    slot_pair = jnp.concatenate([slots, none], axis=1)
    row = iota((place, 16), 0)
    hit = (row // per == pair) & (row % SLOTS == slot_pair)
    values = near_tokens[...].astype(f32)
    values = jnp.concatenate([values, jnp.zeros_like(values)], axis=0).astype(bf16)
    out[...] = dot(jnp.where(hit, 1.0, 0.0).astype(bf16), values).astype(bf16)

    likely = near_probs[...]
    shares = likely / jnp.sum(likely, axis=0, keepdims=True)
    row = iota((2 * place, 8), 0)
    total = jnp.zeros((2 * place, 8), f32)
    for k in range(members.shape[0]):
        member = near_members[k : k + 1, :]
        at = (place_in(BACK_Z, chosen) * (EPG // 2) + place_in(BACK_X, member // 2)) * (2 * SLOTS) + (member % 2) * SLOTS + slots
        total = total + jnp.where(row == at, shares[k : k + 1, :], 0.0)
    weights[...] = jnp.concatenate(three(total), axis=1).astype(bf16)
    affine[...] = by_row(three(near_gain[...]) + three(near_bias[...]), LANES).astype(bf16)


def spread_body(core, arrived, affine, gate, up, kept, given):
    rows = arrived.shape[0]
    values = arrived[...].astype(f32)
    mean = jnp.sum(values, axis=1, keepdims=True) / LANES
    centred = values - mean
    square = jnp.sum(centred * centred, axis=1, keepdims=True)

    lane = iota((rows, LANES), 1)
    stats = jnp.where(lane == 0, mean, jnp.where(lane == 1, square, 0.0))
    stats = jnp.concatenate([stats, jnp.zeros((LANES - rows, LANES), f32)], axis=0).T

    wide = affine[...].astype(f32)
    gain = wide[0:1] + wide[1:2] + wide[2:3]
    left = jnp.concatenate([(centred * gain).astype(bf16), affine[...]], axis=0)
    none = jnp.zeros((1, LANES), f32)
    for out, expert in ((kept, core[0]), (given, 1 - core[0])):
        split = out is given
        for mat, weight in enumerate((gate, up)):
            total = dot(left, weight[expert])
            tail = total[rows : rows + 8]
            gain_sum = tail[0:1] + tail[1:2] + tail[2:3]
            bias_sum = tail[3:4] + tail[4:5] + tail[5:6]
            stat = stats[mat : mat + 1]
            put = slice(mat * LANES, (mat + 1) * LANES)
            for y in range(out.shape[0]):
                lanes = slice(y * LANES, (y + 1) * LANES)
                out[y, 0:rows, put] = total[0:rows, lanes].astype(out.dtype)
                g, b = gain_sum[:, lanes], bias_sum[:, lanes]
                parts = three(g)[0:2] + three(b)[0:2] + three(stat) if split else (g, none, b, none, stat)
                out[y, rows : rows + 8, put] = by_row(parts, LANES).astype(out.dtype)


def merge_body(width, core, kept, both, out):
    tiles, tall, wide = kept.shape
    rows = tall - 8
    peer = 1 - core[0]
    mine, theirs = kept[0, rows:tall, :], both[peer, 0, rows:tall, :].astype(f32)
    theirs = theirs[4:5] + theirs[5:6] + theirs[6:7]
    own_mean, own_square = mine[4:5, 0:LANES], mine[4:5, LANES:]
    other_mean, other_square = theirs[:, 0:LANES], theirs[:, LANES:]
    mean = (own_mean + other_mean) * 0.5
    own_shift, other_shift = own_mean - mean, other_mean - mean
    square = own_square + other_square + width * (own_shift * own_shift + other_shift * other_shift)
    stats = three(jnp.concatenate([mean, square], axis=1))
    turned = jnp.concatenate(
        [by_row([own_shift, other_shift], LANES), jnp.zeros((LANES - 8, LANES), f32)], axis=0
    ).T
    own_shift, other_shift = turned[0:rows, 0:1], turned[0:rows, 1:2]
    for y in range(tiles):
        own_tail, other_tail = kept[y, rows:tall, :], both[peer, y, rows:tall, :].astype(f32)
        own_gain, other_gain = own_tail[0:1], other_tail[0:1] + other_tail[1:2]
        bias = own_tail[2:3] + other_tail[2:3] + other_tail[3:4]
        total = kept[y, 0:rows, :] + both[peer, y, 0:rows, :].astype(f32)
        total = total + own_shift * own_gain + other_shift * other_gain
        out[y, 0:rows, :] = total.astype(bf16)
        parts = three(own_gain + other_gain)[0:2] + three(bias)[0:2] + stats
        out[y, rows:tall, :] = by_row(parts, wide).astype(bf16)


def activate_body(features, parts, out):
    peers = parts.shape[0]
    rows = parts.shape[1] - 8
    tails = [parts[s, rows : rows + 8, :].astype(f32) for s in range(peers)]
    means = by_row([t[4:5, 0:LANES] + t[5:6, 0:LANES] + t[6:7, 0:LANES] for t in tails], LANES)
    squares = by_row([t[4:5, LANES:] + t[5:6, LANES:] + t[6:7, LANES:] for t in tails], LANES)
    center = jnp.sum(means, axis=0, keepdims=True) / peers
    shift = means - center
    spread = jnp.sum(squares + (features // peers) * shift * shift, axis=0, keepdims=True) / features
    scale = jnp.broadcast_to(lax.rsqrt(spread + NORM_EPSILON), (8, LANES))
    turned = jnp.concatenate([shift, scale, jnp.zeros((LANES - 16, LANES), f32)], axis=0).T

    sums = parts[0, 0:rows, :].astype(f32)
    for s in range(1, peers):
        sums = sums + parts[s, 0:rows, :].astype(f32)
    bias = tails[0][2:3] + tails[0][3:4]
    for s in range(peers):
        sums = sums + turned[0:rows, s : s + 1] * (tails[s][0:1] + tails[s][1:2])
        if s:
            bias = bias + tails[s][2:3] + tails[s][3:4]
    full = turned[0:rows, 8:9] * sums + bias
    gate, up = full[:, 0:LANES], full[:, LANES:]
    hidden = (gate / (1.0 + jnp.exp(-gate)) * up).astype(bf16)
    for s in range(peers):
        out[s] = hidden


def project_body(hidden, down, out):
    experts, tiles, rows, width = hidden.shape
    places = out.shape[0]
    row, source = iota((places, places), 0), iota((places, places), 1)
    results = []
    for e in range(experts):
        wide = jnp.concatenate([hidden[e, ROWS_Y.index(y)] for y in SUMS_Y], axis=1)
        results.append(dot(wide, down[e]).astype(bf16))
    expert, slot = source // rows, source % rows
    puts = row == (slot // SLOTS) * (2 * SLOTS) + expert * SLOTS + slot % SLOTS
    out[...] = dot(jnp.where(puts, 1.0, 0.0).astype(bf16), jnp.concatenate(results, axis=0)).astype(bf16)


def combine_body(returned, weights, out):
    count = out.shape[0]
    total = lax.dot_general(
        weights[...], returned[...], (((0,), (0,)), ((), ())), preferred_element_type=f32
    )
    total = total[0:count] + total[count : 2 * count] + total[2 * count :]
    out[...] = total.astype(bf16)


def on_device(
    tokens,
    norm_gain,
    norm_bias,
    group_pick,
    member_pick,
    picked_probs,
    gate_weight,
    up_weight,
    down_weight,
):
    ep = "e"
    peers = lax.axis_size(ep)
    tiles = lax.axis_size("y")
    count, width = tokens.shape
    inner = gate_weight.shape[2]
    rows = peers * SLOTS
    places = 2 * rows
    features = width * tiles * 2
    core = lax.axis_index("c")
    groups, members, probs = group_pick.T, member_pick.T, picked_probs.T

    at = core.reshape(1)
    outgoing, weights, affine = call(
        place_body,
        (shape((rows, LANES)), shape((places, 3 * count)), shape((8, LANES))),
        [SMEM] + [ANY] * 8,
        scratch=[
            pltpu.VMEM(tokens.shape, tokens.dtype),
            pltpu.VMEM(groups.shape, groups.dtype),
            pltpu.VMEM(members.shape, members.dtype),
            pltpu.VMEM(probs.shape, probs.dtype),
            pltpu.VMEM((1, width), f32),
            pltpu.VMEM((1, width), f32),
            pltpu.SemaphoreType.DMA((6,)),
        ],
    )(
        at,
        tokens,
        groups,
        members,
        probs,
        norm_gain.reshape(1, width),
        norm_bias.reshape(1, width),
        gate_weight,
        up_weight,
    )
    arrived = lax.all_to_all(
        outgoing.reshape(peers, SLOTS, LANES), ep, split_axis=0, concat_axis=0, tiled=True, axis_index_groups=[ends(OUT_Z, OUT_X)]
    ).reshape(rows, LANES)

    whole = (tiles, rows + 8, 2 * LANES)
    kept, given = call(
        spread_body,
        (shape(whole, f32), shape(whole)),
        [SMEM] + [VMEM] * 4,
        flops=2 * (rows + 8) * width * 4 * inner,
        moved=gate_weight.size * 4,
    )(at, arrived, affine, gate_weight, up_weight)
    both = lax.all_gather(given, "c", axis=0, tiled=False)
    parts = call(functools.partial(merge_body, width), shape(whole), [SMEM] + [VMEM] * 2)(at, kept, both)
    parts = lax.all_to_all(
        parts, "y", split_axis=0, concat_axis=0, tiled=True, axis_index_groups=[SUMS_Y]
    )
    hidden = call(functools.partial(activate_body, features), shape((tiles, rows, LANES)), [VMEM])(parts)
    hidden = lax.all_to_all(
        hidden, "y", split_axis=0, concat_axis=0, tiled=True, axis_index_groups=[ROWS_Y]
    )
    hidden = lax.all_gather(hidden, "c", axis=0, tiled=False)
    results = call(
        project_body,
        shape((places, LANES)),
        [VMEM] * 2,
        flops=2 * rows * 2 * inner * width,
        moved=down_weight.size * 2,
    )(hidden, down_weight)
    returned = lax.all_to_all(
        results.reshape(peers, 2 * SLOTS, LANES), ep, split_axis=0, concat_axis=0, tiled=True, axis_index_groups=[ends(BACK_Z, BACK_X)]
    ).reshape(places, LANES)
    return call(combine_body, jax.ShapeDtypeStruct((count, LANES), bf16), [VMEM] * 2)(returned, weights)


def solution(mesh):
    finer = Mesh(mesh.devices.reshape(32, 8, 2), ("e", "y", "c"))
    ep, tp = "e", ("y", "c")
    placed = (
        P(ep, tp),
        P(tp),
        P(tp),
        P(ep, None),
        P(ep, None),
        P(ep, None),
        P(ep, tp, None),
        P(ep, tp, None),
        P(ep, None, tp),
    )
    return jax.shard_map(
        on_device, mesh=finer, in_specs=placed, out_specs=P(ep, tp), check_vma=False
    )
```

```python
import functools

import jax
import jax.numpy as jnp
from jax import lax
from jax.experimental import pallas as pl
from jax.experimental.pallas import tpu as pltpu
from jax.sharding import Mesh
from jax.sharding import PartitionSpec as P

f32 = jnp.float32
bf16 = jnp.bfloat16

EPG = 8
SLOTS = 2
LANES = 128
SUMS_Y = [5, 3, 4, 2, 6, 1, 7, 0]
ROWS_Y = [4, 3, 5, 2, 6, 1, 7, 0]
OUT_Z, OUT_X = [4, 3, 5, 2, 6, 1, 7, 0], [2, 1, 3, 0]
BACK_Z, BACK_X = [4, 3, 5, 2, 6, 1, 7, 0], [2, 1, 3, 0]
NORM_EPSILON = 1e-05

VMEM = pl.BlockSpec(memory_space=pltpu.VMEM)
SMEM = pl.BlockSpec(memory_space=pltpu.SMEM)
ANY = pl.BlockSpec(memory_space=pl.ANY)


def call(body, out_shape, in_specs, flops=0, moved=0, scratch=()):
    specs = jax.tree.map(lambda _: VMEM, out_shape)
    kernel = pl.pallas_call(
        body,
        out_shape=out_shape,
        in_specs=in_specs,
        out_specs=specs,
        scratch_shapes=scratch,
        cost_estimate=pl.CostEstimate(flops=flops, bytes_accessed=moved, transcendentals=0),
    )

    def run(*args):
        near = [
            pltpu.with_memory_space_constraint(a, pltpu.VMEM) if spec is VMEM else a
            for a, spec in zip(args, in_specs)
        ]
        return kernel(*near)

    return run


def shape(dims, dtype=bf16):
    return pltpu.VMEM(dims, dtype)


def three(value):
    high = value.astype(bf16).astype(f32)
    middle = (value - high).astype(bf16).astype(f32)
    low = (value - high - middle).astype(bf16).astype(f32)
    return high, middle, low


def iota(dims, axis):
    return lax.broadcasted_iota(jnp.int32, dims, axis)


def place_in(order, values):
    at = jnp.zeros_like(values)
    for i, value in enumerate(order):
        at = jnp.where(values == value, i, at)
    return at


def ends(order_z, order_x):
    return [z * len(order_x) + x for z in order_z for x in order_x]


def by_row(rows, width):
    at = iota((8, width), 0)
    out = jnp.zeros((8, width), f32)
    for i, row in enumerate(rows):
        out = jnp.where(at == i, jnp.broadcast_to(row, (8, width)), out)
    return out


def dot(a, b):
    return jnp.dot(a, b, preferred_element_type=f32)


def slots_of(groups):
    count = groups.shape[1]
    at = iota((1, count), 1)
    slots = jnp.zeros((1, count), jnp.int32)
    for j in range(count - 1):
        same = jnp.broadcast_to(groups[:, j : j + 1], (1, count)) == groups
        slots = slots + jnp.where(same & (at > j), 1, 0)
    return slots


def place_body(core, tokens, groups, members, probs, gain, bias, gate, up, out, weights, affine, *scratch):
    near_tokens, near_groups, near_members, near_probs, near_gain, near_bias, arrived = scratch
    pairs = (
        (groups, near_groups),
        (tokens, near_tokens),
        (members, near_members),
        (probs, near_probs),
        (gain, near_gain),
        (bias, near_bias),
    )
    copies = [pltpu.make_async_copy(a, b, arrived.at[i]) for i, (a, b) in enumerate(pairs)]
    for copy in copies:
        copy.start()
    for copy in copies:
        copy.wait()
    place = out.shape[0]
    per = place // 8
    chosen = near_groups[...]
    slots = slots_of(chosen)
    none = jnp.full((1, 8), -1, jnp.int32)
    pair = jnp.concatenate([place_in(OUT_Z, chosen), none], axis=1)
    slot_pair = jnp.concatenate([slots, none], axis=1)
    row = iota((place, 16), 0)
    hit = (row // per == pair) & (row % SLOTS == slot_pair)
    values = near_tokens[...].astype(f32)
    values = jnp.concatenate([values, jnp.zeros_like(values)], axis=0).astype(bf16)
    out[...] = dot(jnp.where(hit, 1.0, 0.0).astype(bf16), values).astype(bf16)

    likely = near_probs[...]
    shares = likely / jnp.sum(likely, axis=0, keepdims=True)
    row = iota((2 * place, 8), 0)
    total = jnp.zeros((2 * place, 8), f32)
    for k in range(members.shape[0]):
        member = near_members[k : k + 1, :]
        at = (place_in(BACK_Z, chosen) * (EPG // 2) + place_in(BACK_X, member // 2)) * (2 * SLOTS) + (member % 2) * SLOTS + slots
        total = total + jnp.where(row == at, shares[k : k + 1, :], 0.0)
    weights[...] = jnp.concatenate(three(total), axis=1).astype(bf16)
    affine[...] = by_row(three(near_gain[...]) + three(near_bias[...]), LANES).astype(bf16)


def spread_body(core, arrived, affine, gate, up, kept, given):
    rows = arrived.shape[0]
    values = arrived[...].astype(f32)
    mean = jnp.sum(values, axis=1, keepdims=True) / LANES
    centred = values - mean
    square = jnp.sum(centred * centred, axis=1, keepdims=True)

    lane = iota((rows, LANES), 1)
    stats = jnp.where(lane == 0, mean, jnp.where(lane == 1, square, 0.0))
    stats = jnp.concatenate([stats, jnp.zeros((LANES - rows, LANES), f32)], axis=0).T

    wide = affine[...].astype(f32)
    gain = wide[0:1] + wide[1:2] + wide[2:3]
    left = jnp.concatenate([(centred * gain).astype(bf16), affine[...]], axis=0)
    none = jnp.zeros((1, LANES), f32)
    for out, expert in ((kept, core[0]), (given, 1 - core[0])):
        split = out is given
        for mat, weight in enumerate((gate, up)):
            total = dot(left, weight[expert])
            tail = total[rows : rows + 8]
            gain_sum = tail[0:1] + tail[1:2] + tail[2:3]
            bias_sum = tail[3:4] + tail[4:5] + tail[5:6]
            stat = stats[mat : mat + 1]
            put = slice(mat * LANES, (mat + 1) * LANES)
            for y in range(out.shape[0]):
                lanes = slice(y * LANES, (y + 1) * LANES)
                out[y, 0:rows, put] = total[0:rows, lanes].astype(out.dtype)
                g, b = gain_sum[:, lanes], bias_sum[:, lanes]
                parts = three(g)[0:2] + three(b)[0:2] + three(stat) if split else (g, none, b, none, stat)
                out[y, rows : rows + 8, put] = by_row(parts, LANES).astype(out.dtype)


def merge_body(width, core, kept, both, out):
    tiles, tall, wide = kept.shape
    rows = tall - 8
    peer = 1 - core[0]
    mine, theirs = kept[0, rows:tall, :], both[peer, 0, rows:tall, :].astype(f32)
    theirs = theirs[4:5] + theirs[5:6] + theirs[6:7]
    own_mean, own_square = mine[4:5, 0:LANES], mine[4:5, LANES:]
    other_mean, other_square = theirs[:, 0:LANES], theirs[:, LANES:]
    mean = (own_mean + other_mean) * 0.5
    own_shift, other_shift = own_mean - mean, other_mean - mean
    square = own_square + other_square + width * (own_shift * own_shift + other_shift * other_shift)
    stats = three(jnp.concatenate([mean, square], axis=1))
    turned = jnp.concatenate(
        [by_row([own_shift, other_shift], LANES), jnp.zeros((LANES - 8, LANES), f32)], axis=0
    ).T
    own_shift, other_shift = turned[0:rows, 0:1], turned[0:rows, 1:2]
    for y in range(tiles):
        own_tail, other_tail = kept[y, rows:tall, :], both[peer, y, rows:tall, :].astype(f32)
        own_gain, other_gain = own_tail[0:1], other_tail[0:1] + other_tail[1:2]
        bias = own_tail[2:3] + other_tail[2:3] + other_tail[3:4]
        total = kept[y, 0:rows, :] + both[peer, y, 0:rows, :].astype(f32)
        total = total + own_shift * own_gain + other_shift * other_gain
        out[y, 0:rows, :] = total.astype(bf16)
        parts = three(own_gain + other_gain)[0:2] + three(bias)[0:2] + stats
        out[y, rows:tall, :] = by_row(parts, wide).astype(bf16)


def activate_body(features, parts, out):
    peers = parts.shape[0]
    rows = parts.shape[1] - 8
    tails = [parts[s, rows : rows + 8, :].astype(f32) for s in range(peers)]
    means = by_row([t[4:5, 0:LANES] + t[5:6, 0:LANES] + t[6:7, 0:LANES] for t in tails], LANES)
    squares = by_row([t[4:5, LANES:] + t[5:6, LANES:] + t[6:7, LANES:] for t in tails], LANES)
    center = jnp.sum(means, axis=0, keepdims=True) / peers
    shift = means - center
    spread = jnp.sum(squares + (features // peers) * shift * shift, axis=0, keepdims=True) / features
    scale = jnp.broadcast_to(lax.rsqrt(spread + NORM_EPSILON), (8, LANES))
    turned = jnp.concatenate([shift, scale, jnp.zeros((LANES - 16, LANES), f32)], axis=0).T

    sums = parts[0, 0:rows, :].astype(f32)
    for s in range(1, peers):
        sums = sums + parts[s, 0:rows, :].astype(f32)
    bias = tails[0][2:3] + tails[0][3:4]
    for s in range(peers):
        sums = sums + turned[0:rows, s : s + 1] * (tails[s][0:1] + tails[s][1:2])
        if s:
            bias = bias + tails[s][2:3] + tails[s][3:4]
    full = turned[0:rows, 8:9] * sums + bias
    gate, up = full[:, 0:LANES], full[:, LANES:]
    hidden = (gate / (1.0 + jnp.exp(-gate)) * up).astype(bf16)
    for s in range(peers):
        out[s] = hidden


def project_body(hidden, down, out):
    experts, tiles, rows, width = hidden.shape
    places = out.shape[0]
    row, source = iota((places, rows), 0), iota((places, rows), 1)
    total = jnp.zeros((places, LANES), f32)
    for e in range(experts):
        wide = jnp.concatenate([hidden[e, ROWS_Y.index(y)] for y in SUMS_Y], axis=1)
        result = dot(wide, down[e]).astype(bf16)
        puts = row == (source // SLOTS) * (2 * SLOTS) + e * SLOTS + source % SLOTS
        total = total + dot(jnp.where(puts, 1.0, 0.0).astype(bf16), result)
    out[...] = total.astype(bf16)


def combine_body(returned, weights, out):
    count = out.shape[0]
    total = lax.dot_general(
        weights[...], returned[...], (((0,), (0,)), ((), ())), preferred_element_type=f32
    )
    total = total[0:count] + total[count : 2 * count] + total[2 * count :]
    out[...] = total.astype(bf16)


def on_device(
    tokens,
    norm_gain,
    norm_bias,
    group_pick,
    member_pick,
    picked_probs,
    gate_weight,
    up_weight,
    down_weight,
):
    ep = "e"
    peers = lax.axis_size(ep)
    tiles = lax.axis_size("y")
    count, width = tokens.shape
    inner = gate_weight.shape[2]
    rows = peers * SLOTS
    places = 2 * rows
    features = width * tiles * 2
    core = lax.axis_index("c")
    groups, members, probs = group_pick.T, member_pick.T, picked_probs.T

    at = core.reshape(1)
    outgoing, weights, affine = call(
        place_body,
        (shape((rows, LANES)), shape((places, 3 * count)), shape((8, LANES))),
        [SMEM] + [ANY] * 8,
        scratch=[
            pltpu.VMEM(tokens.shape, tokens.dtype),
            pltpu.VMEM(groups.shape, groups.dtype),
            pltpu.VMEM(members.shape, members.dtype),
            pltpu.VMEM(probs.shape, probs.dtype),
            pltpu.VMEM((1, width), f32),
            pltpu.VMEM((1, width), f32),
            pltpu.SemaphoreType.DMA((6,)),
        ],
    )(
        at,
        tokens,
        groups,
        members,
        probs,
        norm_gain.reshape(1, width),
        norm_bias.reshape(1, width),
        gate_weight,
        up_weight,
    )
    arrived = lax.all_to_all(
        outgoing.reshape(peers, SLOTS, LANES), ep, split_axis=0, concat_axis=0, tiled=True, axis_index_groups=[ends(OUT_Z, OUT_X)]
    ).reshape(rows, LANES)

    whole = (tiles, rows + 8, 2 * LANES)
    kept, given = call(
        spread_body,
        (shape(whole, f32), shape(whole)),
        [SMEM] + [VMEM] * 4,
        flops=2 * (rows + 8) * width * 4 * inner,
        moved=gate_weight.size * 4,
    )(at, arrived, affine, gate_weight, up_weight)
    both = lax.all_gather(given, "c", axis=0, tiled=False)
    parts = call(functools.partial(merge_body, width), shape(whole), [SMEM] + [VMEM] * 2)(at, kept, both)
    parts = lax.all_to_all(
        parts, "y", split_axis=0, concat_axis=0, tiled=True, axis_index_groups=[SUMS_Y]
    )
    hidden = call(functools.partial(activate_body, features), shape((tiles, rows, LANES)), [VMEM])(parts)
    hidden = lax.all_to_all(
        hidden, "y", split_axis=0, concat_axis=0, tiled=True, axis_index_groups=[ROWS_Y]
    )
    hidden = lax.all_gather(hidden, "c", axis=0, tiled=False)
    results = call(
        project_body,
        shape((places, LANES)),
        [VMEM] * 2,
        flops=2 * rows * 2 * inner * width,
        moved=down_weight.size * 2,
    )(hidden, down_weight)
    returned = lax.all_to_all(
        results.reshape(peers, 2 * SLOTS, LANES), ep, split_axis=0, concat_axis=0, tiled=True, axis_index_groups=[ends(BACK_Z, BACK_X)]
    ).reshape(places, LANES)
    return call(combine_body, jax.ShapeDtypeStruct((count, LANES), bf16), [VMEM] * 2)(returned, weights)


def solution(mesh):
    finer = Mesh(mesh.devices.reshape(32, 8, 2), ("e", "y", "c"))
    ep, tp = "e", ("y", "c")
    placed = (
        P(ep, tp),
        P(tp),
        P(tp),
        P(ep, None),
        P(ep, None),
        P(ep, None),
        P(ep, tp, None),
        P(ep, tp, None),
        P(ep, None, tp),
    )
    return jax.shard_map(
        on_device, mesh=finer, in_specs=placed, out_specs=P(ep, tp), check_vma=False
    )
```

```python
import functools

import jax
import jax.numpy as jnp
from jax import lax
from jax.experimental import pallas as pl
from jax.experimental.pallas import tpu as pltpu
from jax.sharding import Mesh
from jax.sharding import PartitionSpec as P

f32 = jnp.float32
bf16 = jnp.bfloat16

EPG = 8
SLOTS = 2
LANES = 128
SUMS_Y = [4, 3, 5, 2, 6, 1, 7, 0]
ROWS_Y = [4, 3, 5, 2, 6, 1, 7, 0]
OUT_Z, OUT_X = [4, 3, 5, 2, 6, 1, 7, 0], [2, 1, 3, 0]
BACK_Z, BACK_X = [4, 3, 5, 2, 6, 1, 7, 0], [2, 1, 3, 0]
NORM_EPSILON = 1e-05

VMEM = pl.BlockSpec(memory_space=pltpu.VMEM)
SMEM = pl.BlockSpec(memory_space=pltpu.SMEM)
ANY = pl.BlockSpec(memory_space=pl.ANY)


def call(body, out_shape, in_specs, flops=0, moved=0, scratch=()):
    specs = jax.tree.map(lambda _: VMEM, out_shape)
    kernel = pl.pallas_call(
        body,
        out_shape=out_shape,
        in_specs=in_specs,
        out_specs=specs,
        scratch_shapes=scratch,
        cost_estimate=pl.CostEstimate(flops=flops, bytes_accessed=moved, transcendentals=0),
    )

    def run(*args):
        near = [
            pltpu.with_memory_space_constraint(a, pltpu.VMEM) if spec is VMEM else a
            for a, spec in zip(args, in_specs)
        ]
        return kernel(*near)

    return run


def shape(dims, dtype=bf16):
    return pltpu.VMEM(dims, dtype)


def three(value):
    high = value.astype(bf16).astype(f32)
    middle = (value - high).astype(bf16).astype(f32)
    low = (value - high - middle).astype(bf16).astype(f32)
    return high, middle, low


def iota(dims, axis):
    return lax.broadcasted_iota(jnp.int32, dims, axis)


def place_in(order, values):
    at = jnp.zeros_like(values)
    for i, value in enumerate(order):
        at = jnp.where(values == value, i, at)
    return at


def ends(order_z, order_x):
    return [z * len(order_x) + x for z in order_z for x in order_x]


def by_row(rows, width):
    at = iota((8, width), 0)
    out = jnp.zeros((8, width), f32)
    for i, row in enumerate(rows):
        out = jnp.where(at == i, jnp.broadcast_to(row, (8, width)), out)
    return out


def dot(a, b):
    return jnp.dot(a, b, preferred_element_type=f32)


def slots_of(groups):
    count = groups.shape[1]
    at = iota((1, count), 1)
    slots = jnp.zeros((1, count), jnp.int32)
    for j in range(count - 1):
        same = jnp.broadcast_to(groups[:, j : j + 1], (1, count)) == groups
        slots = slots + jnp.where(same & (at > j), 1, 0)
    return slots


def place_body(core, tokens, groups, members, probs, gain, bias, gate, up, out, weights, affine, *scratch):
    near_tokens, near_groups, near_members, near_probs, near_gain, near_bias, arrived = scratch
    pairs = (
        (groups, near_groups),
        (tokens, near_tokens),
        (members, near_members),
        (probs, near_probs),
        (gain, near_gain),
        (bias, near_bias),
    )
    copies = [pltpu.make_async_copy(a, b, arrived.at[i]) for i, (a, b) in enumerate(pairs)]
    for copy in copies:
        copy.start()
    for copy in copies:
        copy.wait()
    place = out.shape[0]
    per = place // 8
    chosen = near_groups[...]
    slots = slots_of(chosen)
    none = jnp.full((1, 8), -1, jnp.int32)
    pair = jnp.concatenate([place_in(OUT_Z, chosen), none], axis=1)
    slot_pair = jnp.concatenate([slots, none], axis=1)
    row = iota((place, 16), 0)
    hit = (row // per == pair) & (row % SLOTS == slot_pair)
    values = near_tokens[...].astype(f32)
    values = jnp.concatenate([values, jnp.zeros_like(values)], axis=0).astype(bf16)
    out[...] = dot(jnp.where(hit, 1.0, 0.0).astype(bf16), values).astype(bf16)

    likely = near_probs[...]
    shares = likely / jnp.sum(likely, axis=0, keepdims=True)
    row = iota((2 * place, 8), 0)
    total = jnp.zeros((2 * place, 8), f32)
    for k in range(members.shape[0]):
        member = near_members[k : k + 1, :]
        at = (place_in(BACK_Z, chosen) * (EPG // 2) + place_in(BACK_X, member // 2)) * (2 * SLOTS) + (member % 2) * SLOTS + slots
        total = total + jnp.where(row == at, shares[k : k + 1, :], 0.0)
    weights[...] = jnp.concatenate(three(total)[0:2], axis=1).astype(bf16)
    affine[...] = by_row(three(near_gain[...]) + three(near_bias[...]), LANES).astype(bf16)


def spread_body(core, arrived, affine, gate, up, kept, given):
    rows = arrived.shape[0]
    values = arrived[...].astype(f32)
    mean = jnp.sum(values, axis=1, keepdims=True) / LANES
    centred = values - mean
    square = jnp.sum(centred * centred, axis=1, keepdims=True)

    lane = iota((rows, LANES), 1)
    stats = jnp.where(lane == 0, mean, jnp.where(lane == 1, square, 0.0))
    stats = jnp.concatenate([stats, jnp.zeros((LANES - rows, LANES), f32)], axis=0).T

    wide = affine[...].astype(f32)
    gain = wide[0:1] + wide[1:2] + wide[2:3]
    left = jnp.concatenate([(centred * gain).astype(bf16), affine[...]], axis=0)
    none = jnp.zeros((1, LANES), f32)
    for out, expert in ((kept, core[0]), (given, 1 - core[0])):
        split = out is given
        for mat, weight in enumerate((gate, up)):
            total = dot(left, weight[expert])
            tail = total[rows : rows + 8]
            gain_sum = tail[0:1] + tail[1:2] + tail[2:3]
            bias_sum = tail[3:4] + tail[4:5] + tail[5:6]
            stat = stats[mat : mat + 1]
            put = slice(mat * LANES, (mat + 1) * LANES)
            for y in range(out.shape[0]):
                lanes = slice(y * LANES, (y + 1) * LANES)
                out[y, 0:rows, put] = total[0:rows, lanes].astype(out.dtype)
                g, b = gain_sum[:, lanes], bias_sum[:, lanes]
                parts = three(g)[0:2] + three(b)[0:2] + three(stat) if split else (g, none, b, none, stat)
                out[y, rows : rows + 8, put] = by_row(parts, LANES).astype(out.dtype)


def merge_body(width, core, kept, both, out):
    tiles, tall, wide = kept.shape
    rows = tall - 8
    peer = 1 - core[0]
    mine, theirs = kept[0, rows:tall, :], both[peer, 0, rows:tall, :].astype(f32)
    theirs = theirs[4:5] + theirs[5:6] + theirs[6:7]
    own_mean, own_square = mine[4:5, 0:LANES], mine[4:5, LANES:]
    other_mean, other_square = theirs[:, 0:LANES], theirs[:, LANES:]
    mean = (own_mean + other_mean) * 0.5
    own_shift, other_shift = own_mean - mean, other_mean - mean
    square = own_square + other_square + width * (own_shift * own_shift + other_shift * other_shift)
    stats = three(jnp.concatenate([mean, square], axis=1))
    turned = jnp.concatenate(
        [by_row([own_shift, other_shift], LANES), jnp.zeros((LANES - 8, LANES), f32)], axis=0
    ).T
    own_shift, other_shift = turned[0:rows, 0:1], turned[0:rows, 1:2]
    for y in range(tiles):
        own_tail, other_tail = kept[y, rows:tall, :], both[peer, y, rows:tall, :].astype(f32)
        own_gain, other_gain = own_tail[0:1], other_tail[0:1] + other_tail[1:2]
        bias = own_tail[2:3] + other_tail[2:3] + other_tail[3:4]
        total = kept[y, 0:rows, :] + both[peer, y, 0:rows, :].astype(f32)
        total = total + own_shift * own_gain + other_shift * other_gain
        out[y, 0:rows, :] = total.astype(bf16)
        parts = three(own_gain + other_gain)[0:2] + three(bias)[0:2] + stats
        out[y, rows:tall, :] = by_row(parts, wide).astype(bf16)


def activate_body(features, parts, out):
    peers = parts.shape[0]
    rows = parts.shape[1] - 8
    tails = [parts[s, rows : rows + 8, :].astype(f32) for s in range(peers)]
    means = by_row([t[4:5, 0:LANES] + t[5:6, 0:LANES] + t[6:7, 0:LANES] for t in tails], LANES)
    squares = by_row([t[4:5, LANES:] + t[5:6, LANES:] + t[6:7, LANES:] for t in tails], LANES)
    center = jnp.sum(means, axis=0, keepdims=True) / peers
    shift = means - center
    spread = jnp.sum(squares + (features // peers) * shift * shift, axis=0, keepdims=True) / features
    scale = jnp.broadcast_to(lax.rsqrt(spread + NORM_EPSILON), (8, LANES))
    turned = jnp.concatenate([shift, scale, jnp.zeros((LANES - 16, LANES), f32)], axis=0).T

    sums = parts[0, 0:rows, :].astype(f32)
    for s in range(1, peers):
        sums = sums + parts[s, 0:rows, :].astype(f32)
    bias = tails[0][2:3] + tails[0][3:4]
    for s in range(peers):
        sums = sums + turned[0:rows, s : s + 1] * (tails[s][0:1] + tails[s][1:2])
        if s:
            bias = bias + tails[s][2:3] + tails[s][3:4]
    full = turned[0:rows, 8:9] * sums + bias
    gate, up = full[:, 0:LANES], full[:, LANES:]
    hidden = (gate / (1.0 + jnp.exp(-gate)) * up).astype(bf16)
    for s in range(peers):
        out[s] = hidden


def project_body(hidden, down, out):
    experts, tiles, rows, width = hidden.shape
    places = out.shape[0]
    row, source = iota((places, rows), 0), iota((places, rows), 1)
    total = jnp.zeros((places, LANES), f32)
    for e in range(experts):
        wide = jnp.concatenate([hidden[e, ROWS_Y.index(y)] for y in SUMS_Y], axis=1)
        result = dot(wide, down[e]).astype(bf16)
        puts = row == (source // SLOTS) * (2 * SLOTS) + e * SLOTS + source % SLOTS
        total = total + dot(jnp.where(puts, 1.0, 0.0).astype(bf16), result)
    out[...] = total.astype(bf16)


def combine_body(returned, weights, out):
    count = out.shape[0]
    total = lax.dot_general(
        weights[...], returned[...], (((0,), (0,)), ((), ())), preferred_element_type=f32
    )
    total = total[0:count] + total[count:]
    out[...] = total.astype(bf16)


def on_device(
    tokens,
    norm_gain,
    norm_bias,
    group_pick,
    member_pick,
    picked_probs,
    gate_weight,
    up_weight,
    down_weight,
):
    ep = "e"
    peers = lax.axis_size(ep)
    tiles = lax.axis_size("y")
    count, width = tokens.shape
    inner = gate_weight.shape[2]
    rows = peers * SLOTS
    places = 2 * rows
    features = width * tiles * 2
    core = lax.axis_index("c")
    groups, members, probs = group_pick.T, member_pick.T, picked_probs.T

    at = core.reshape(1)
    outgoing, weights, affine = call(
        place_body,
        (shape((rows, LANES)), shape((places, 2 * count)), shape((8, LANES))),
        [SMEM] + [ANY] * 8,
        scratch=[
            pltpu.VMEM(tokens.shape, tokens.dtype),
            pltpu.VMEM(groups.shape, groups.dtype),
            pltpu.VMEM(members.shape, members.dtype),
            pltpu.VMEM(probs.shape, probs.dtype),
            pltpu.VMEM((1, width), f32),
            pltpu.VMEM((1, width), f32),
            pltpu.SemaphoreType.DMA((6,)),
        ],
    )(
        at,
        tokens,
        groups,
        members,
        probs,
        norm_gain.reshape(1, width),
        norm_bias.reshape(1, width),
        gate_weight,
        up_weight,
    )
    arrived = lax.all_to_all(
        outgoing.reshape(peers, SLOTS, LANES), ep, split_axis=0, concat_axis=0, tiled=True, axis_index_groups=[ends(OUT_Z, OUT_X)]
    ).reshape(rows, LANES)

    whole = (tiles, rows + 8, 2 * LANES)
    kept, given = call(
        spread_body,
        (shape(whole, f32), shape(whole)),
        [SMEM] + [VMEM] * 4,
        flops=2 * (rows + 8) * width * 4 * inner,
        moved=gate_weight.size * 4,
    )(at, arrived, affine, gate_weight, up_weight)
    both = lax.all_gather(given, "c", axis=0, tiled=False)
    parts = call(functools.partial(merge_body, width), shape(whole), [SMEM] + [VMEM] * 2)(at, kept, both)
    parts = lax.all_to_all(
        parts, "y", split_axis=0, concat_axis=0, tiled=True, axis_index_groups=[SUMS_Y]
    )
    hidden = call(functools.partial(activate_body, features), shape((tiles, rows, LANES)), [VMEM])(parts)
    hidden = lax.all_to_all(
        hidden, "y", split_axis=0, concat_axis=0, tiled=True, axis_index_groups=[ROWS_Y]
    )
    hidden = lax.all_gather(hidden, "c", axis=0, tiled=False)
    results = call(
        project_body,
        shape((places, LANES)),
        [VMEM] * 2,
        flops=2 * rows * 2 * inner * width,
        moved=down_weight.size * 2,
    )(hidden, down_weight)
    returned = lax.all_to_all(
        results.reshape(peers, 2 * SLOTS, LANES), ep, split_axis=0, concat_axis=0, tiled=True, axis_index_groups=[ends(BACK_Z, BACK_X)]
    ).reshape(places, LANES)
    return call(combine_body, jax.ShapeDtypeStruct((count, LANES), bf16), [VMEM] * 2)(returned, weights)


def solution(mesh):
    finer = Mesh(mesh.devices.reshape(32, 8, 2), ("e", "y", "c"))
    ep, tp = "e", ("y", "c")
    placed = (
        P(ep, tp),
        P(tp),
        P(tp),
        P(ep, None),
        P(ep, None),
        P(ep, None),
        P(ep, tp, None),
        P(ep, tp, None),
        P(ep, None, tp),
    )
    return jax.shard_map(
        on_device, mesh=finer, in_specs=placed, out_specs=P(ep, tp), check_vma=False
    )
```
